256 devices in a mesh: sp: 32 (over z, y), tp: 8 (over x, core).
Axes of the slice: x: 4, y: 4, z: 8, core: 2. Of those that a mesh axis runs over, the one named last changes fastest.
Arguments:
- stream: bfloat16 [24576, 2048], P(('sp', 'tp')), may hold values from -6 to 6
- query_first: bfloat16 [24576, 1024], P('sp', 'tp'), may hold values from -6 to 6
- key_first: bfloat16 [24576, 1024], P('sp', 'tp'), may hold values from -6 to 6
- value_first: bfloat16 [24576, 1024], P('sp', 'tp'), may hold values from -6 to 6
- decay_first: bfloat16 [24576, 1024], P('sp', 'tp'), may hold values from -16 to 1
- learning_first: bfloat16 [24576, 1024], P('sp', 'tp'), may hold values from -16 to 4
- output_gate_first: bfloat16 [24576, 1024], P('sp', 'tp'), may hold values from -6 to 6
- extra_decay_first: float32 [24576, 16], P('sp', 'tp'), may hold values from -1 to 0
- head_norm_gain_first: float32 [1024], P('tp'), may hold values from 0.1 to 1.9
- self_weight_first: float32 [1024], P('tp'), may hold values from -0.9 to 0.9
- query_second: bfloat16 [24576, 1024], P('sp', 'tp'), may hold values from -6 to 6
- key_second: bfloat16 [24576, 1024], P('sp', 'tp'), may hold values from -6 to 6
- value_second: bfloat16 [24576, 1024], P('sp', 'tp'), may hold values from -6 to 6
- decay_second: bfloat16 [24576, 1024], P('sp', 'tp'), may hold values from -16 to 1
- learning_second: bfloat16 [24576, 1024], P('sp', 'tp'), may hold values from -16 to 4
- output_gate_second: bfloat16 [24576, 1024], P('sp', 'tp'), may hold values from -6 to 6
- extra_decay_second: float32 [24576, 8], P('sp', 'tp'), may hold values from -1 to 0
- head_norm_gain_second: float32 [1024], P('tp'), may hold values from 0.1 to 1.9
- self_weight_second: float32 [1024], P('tp'), may hold values from -0.9 to 0.9
- output_projection_first: bfloat16 [1024, 2048], replicated, may hold values from -0.125 to 0.125
- output_projection_second: bfloat16 [1024, 2048], replicated, may hold values from -0.125 to 0.125
- middle_norm_gain: float32 [2048], replicated, may hold values from 0.1 to 1.9
- mixer_up_weight: bfloat16 [2048, 8192], P('sp', 'tp'), may hold values from -0.125 to 0.125
- mixer_down_weight: bfloat16 [8192, 2048], P('tp', 'sp'), may hold values from -0.0625 to 0.0625
- final_norm_gain: float32 [2048], replicated, may hold values from 0.1 to 1.9
Outputs:
- result: bfloat16 [24576, 2048], P(('sp', 'tp'))
The draws below stay inside these ranges and needn't reach their ends.
All inputs are finite; a program needn't handle non-finite values.
Results may differ from the reference program's by a relative error of at most 0.019.
Values may be sent and summed in bfloat16 or wider, within the bound.
No kernel may reach another device: no remote copies, remote signals or barrier semaphores. Data moves between devices by JAX's collectives and lax.ppermute only.
A program may use at most 128 MiB of HBM per device.

```python
import jax
import jax.numpy as jnp
from jax import lax

D = 2048
FF = 8192
FIRST_HEADS = 16
FIRST_HEAD_SIZE = 64
SECOND_HEADS = 8
SECOND_HEAD_SIZE = 128
TOK_DEV = 768
TOKENS = 24576
N_TP = 8


def head_kinds(key, number_heads, group_label):
    picker = jax.random.fold_in(key, group_label)
    return jax.random.randint(picker, (number_heads,), 0, 2) == 1


def decay_field(key, number_heads, head_dimension_size, group_label):
    quick = head_kinds(key, number_heads, group_label)
    subkeys = jax.random.split(jax.random.fold_in(key, group_label + 100), 3)
    base_level = jnp.where(quick, -3.2, -jnp.log(jnp.float32(TOKENS)) - 1.0)
    jitter = jax.random.uniform(subkeys[0], (number_heads, head_dimension_size), jnp.float32, -0.5, 0.5)
    offset = jax.random.uniform(subkeys[1], (TOKENS // TOK_DEV,), jnp.float32, -0.7, 0.7)
    noise_part = jnp.clip(0.5 * jax.random.normal(subkeys[2], (TOKENS, number_heads * head_dimension_size), jnp.float32), -1.5, 1.5)
    field = (base_level[:, None] + jitter).reshape(1, -1) + jnp.repeat(offset, TOK_DEV)[:, None] + noise_part
    return field.astype(jnp.bfloat16)


def rate_field(key, number_heads, head_dimension_size, group_label):
    quick = head_kinds(key, number_heads, group_label)
    subkey = jax.random.fold_in(key, group_label + 200)
    centre = jnp.where(quick, -1.0, jnp.log(jnp.float32(head_dimension_size) / TOKENS) - 1.0)
    centre = jnp.repeat(centre, head_dimension_size)[None, :]
    noise_part = jnp.clip(jax.random.normal(subkey, (TOKENS, number_heads * head_dimension_size), jnp.float32), -3.0, 3.0)
    return (centre + noise_part).astype(jnp.bfloat16)


def extra_decay_grid(key, number_heads, group_label):
    subkeys = jax.random.split(jax.random.fold_in(key, group_label + 300), 2)
    spots = jax.random.randint(subkeys[0], (3, number_heads), 0, TOKENS)
    depth = jnp.log(jax.random.uniform(subkeys[1], (3, number_heads), jnp.float32, 0.5, 0.8))
    places = jnp.arange(TOKENS)[:, None, None]
    return jnp.sum(jnp.where(places == spots[None], depth[None], 0.0), axis=1).astype(jnp.float32)


def draw_decay_first(key, part):
    return decay_field(key, FIRST_HEADS, FIRST_HEAD_SIZE, 11)


def draw_decay_second(key, part):
    return decay_field(key, SECOND_HEADS, SECOND_HEAD_SIZE, 23)


def draw_learning_first(key, part):
    return rate_field(key, FIRST_HEADS, FIRST_HEAD_SIZE, 11)


def draw_learning_second(key, part):
    return rate_field(key, SECOND_HEADS, SECOND_HEAD_SIZE, 23)


def draw_extra_decay_first(key, part):
    return extra_decay_grid(key, FIRST_HEADS, 11)


def draw_extra_decay_second(key, part):
    return extra_decay_grid(key, SECOND_HEADS, 23)


def block_scale(own_key, shape, pieces, smallest, top_value):
    def one(axis_at, shards_of):
        heights = jax.random.uniform(jax.random.fold_in(jax.random.fold_in(own_key, 6), axis_at), (shards_of,), jnp.float32, smallest / len(pieces), top_value / len(pieces))
        return jnp.repeat(jnp.exp(heights), shape[axis_at] // shards_of).reshape((-1,) + (1,) * (len(shape) - axis_at - 1))

    factor_of = one(*pieces[0])
    for cut in pieces[1:]:
        factor_of = factor_of * one(*cut)
    return factor_of


def scatter_about(stream_key, extent, scale, bound, cuts=(), kind=jnp.bfloat16):
    factor_of = block_scale(stream_key, extent, cuts, -0.22, 0.18) if cuts else 1.0
    values = jax.random.normal(stream_key, extent, jnp.float32) * scale * factor_of
    return jnp.minimum(jnp.maximum(values, -bound), bound).astype(kind)


def setup_inputs(seed: int = 0) -> dict:
    arg_keys = jax.random.split(jax.random.key(seed), 26)
    return {
        "stream": scatter_about(arg_keys[0], (TOKENS, D), 1.0, 6.0, ((0, 256),)),
        "query_first": scatter_about(arg_keys[1], (TOKENS, FIRST_HEADS * FIRST_HEAD_SIZE), 1.0, 6.0, ((0, 32), (1, 8))),
        "key_first": scatter_about(arg_keys[2], (TOKENS, FIRST_HEADS * FIRST_HEAD_SIZE), 1.0, 6.0, ((0, 32), (1, 8))),
        "value_first": scatter_about(arg_keys[3], (TOKENS, FIRST_HEADS * FIRST_HEAD_SIZE), 1.0, 6.0, ((0, 32), (1, 8))),
        "decay_first": draw_decay_first(jax.random.fold_in(arg_keys[25], 71), 0),
        "learning_first": draw_learning_first(jax.random.fold_in(arg_keys[25], 71), 0),
        "output_gate_first": scatter_about(arg_keys[6], (TOKENS, FIRST_HEADS * FIRST_HEAD_SIZE), 1.0, 6.0, ((0, 32), (1, 8))),
        "extra_decay_first": draw_extra_decay_first(jax.random.fold_in(arg_keys[25], 71), 0),
        "head_norm_gain_first": jnp.clip(1.0 + 0.18 * jax.random.normal(arg_keys[8], (FIRST_HEADS * FIRST_HEAD_SIZE,), jnp.float32), 0.1, 1.9),
        "self_weight_first": scatter_about(arg_keys[9], (FIRST_HEADS * FIRST_HEAD_SIZE,), 0.15, 0.9, ((0, 8),), jnp.float32),
        "query_second": scatter_about(arg_keys[10], (TOKENS, SECOND_HEADS * SECOND_HEAD_SIZE), 1.0, 6.0, ((0, 32), (1, 8))),
        "key_second": scatter_about(arg_keys[11], (TOKENS, SECOND_HEADS * SECOND_HEAD_SIZE), 1.0, 6.0, ((0, 32), (1, 8))),
        "value_second": scatter_about(arg_keys[12], (TOKENS, SECOND_HEADS * SECOND_HEAD_SIZE), 1.0, 6.0, ((0, 32), (1, 8))),
        "decay_second": draw_decay_second(jax.random.fold_in(arg_keys[25], 71), 0),
        "learning_second": draw_learning_second(jax.random.fold_in(arg_keys[25], 71), 0),
        "output_gate_second": scatter_about(arg_keys[15], (TOKENS, SECOND_HEADS * SECOND_HEAD_SIZE), 1.0, 6.0, ((0, 32), (1, 8))),
        "extra_decay_second": draw_extra_decay_second(jax.random.fold_in(arg_keys[25], 71), 0),
        "head_norm_gain_second": jnp.clip(1.0 + 0.18 * jax.random.normal(arg_keys[17], (SECOND_HEADS * SECOND_HEAD_SIZE,), jnp.float32), 0.1, 1.9),
        "self_weight_second": scatter_about(arg_keys[18], (SECOND_HEADS * SECOND_HEAD_SIZE,), 0.15, 0.9, ((0, 8),), jnp.float32),
        "output_projection_first": scatter_about(arg_keys[19], (FIRST_HEADS * FIRST_HEAD_SIZE, D), (FIRST_HEADS * FIRST_HEAD_SIZE + SECOND_HEADS * SECOND_HEAD_SIZE) ** -0.5, 0.125),
        "output_projection_second": scatter_about(arg_keys[20], (SECOND_HEADS * SECOND_HEAD_SIZE, D), (FIRST_HEADS * FIRST_HEAD_SIZE + SECOND_HEADS * SECOND_HEAD_SIZE) ** -0.5, 0.125),
        "middle_norm_gain": jnp.clip(1.0 + 0.18 * jax.random.normal(arg_keys[21], (D,), jnp.float32), 0.1, 1.9),
        "mixer_up_weight": scatter_about(arg_keys[22], (D, FF), D ** -0.5, 0.125, ((0, 32), (1, 8))),
        "mixer_down_weight": scatter_about(arg_keys[23], (FF, D), FF ** -0.5, 0.0625, ((0, 8), (1, 32))),
        "final_norm_gain": jnp.clip(1.0 + 0.18 * jax.random.normal(arg_keys[24], (D,), jnp.float32), 0.1, 1.9),
    }


EPS_KEY = 1e-05
EPS_HEAD = 0.00064
EPS_NORM = 1e-05
ALPHA = 2.0 ** 0.25

def normalize(value_inputs, gain):
    mean_part = lax.optimization_barrier(jnp.mean(value_inputs, -1, keepdims=True))
    spread = lax.optimization_barrier(jnp.mean(jnp.square(value_inputs - mean_part), -1, keepdims=True))
    return (value_inputs - mean_part) * lax.rsqrt(spread + EPS_NORM) * gain

def feature_rows(query_input, key_inputs, value_inputs, decay_input, learning_input, extra_decay, head_dimension_size):
    tok_count = query_input.shape[0]
    number_heads = query_input.shape[1] // head_dimension_size

    def reshaped(array):
        return array.astype(jnp.float32).reshape(tok_count, number_heads, head_dimension_size)
    query_matrix, key_matrix, value_matrix = (reshaped(query_input), reshaped(key_inputs), reshaped(value_inputs))
    normalized = key_matrix * lax.rsqrt(lax.optimization_barrier(jnp.mean(key_matrix * key_matrix, -1, keepdims=True)) + EPS_KEY) * head_dimension_size ** (-0.5)
    learning_rate = jax.nn.sigmoid(reshaped(learning_input))
    log_decay = -jnp.exp(-jax.nn.softplus(-reshaped(decay_input)) - 0.5) + extra_decay[:, :, None]
    return (query_matrix, key_matrix, value_matrix, normalized, learning_rate, log_decay)

def head_result(head_shaped, query_matrix, key_matrix, value_matrix, output_gate, head_norm_gain, self_weight, head_dimension_size):
    mean_part = lax.optimization_barrier(jnp.mean(head_shaped, -1, keepdims=True))
    spread = lax.optimization_barrier(jnp.mean(jnp.square(head_shaped - mean_part), -1, keepdims=True))
    normalized = (head_shaped - mean_part) * lax.rsqrt(spread + EPS_HEAD) * head_norm_gain.reshape(-1, head_dimension_size)
    additional = lax.optimization_barrier(jnp.sum(query_matrix * key_matrix * self_weight.reshape(-1, head_dimension_size), -1, keepdims=True)) * value_matrix
    gated = (normalized + additional) * jax.nn.sigmoid(output_gate.astype(jnp.float32).reshape(head_shaped.shape))
    return gated.reshape(head_shaped.shape[0], -1).astype(jnp.bfloat16)

def apply_group(query_input, key_inputs, value_inputs, decay_input, learning_input, extra_decay, output_gate, head_norm_gain, self_weight, head_dimension_size):
    query_matrix, key_matrix, value_matrix, normalized, learning_rate, log_decay = feature_rows(query_input, key_inputs, value_inputs, decay_input, learning_input, extra_decay, head_dimension_size)
    number_heads = query_matrix.shape[1]

    def advance(recurrent_state, inputs):
        query_now, key_now, value_now, normed_now, learn_now, logdec_now = inputs
        recall = jnp.einsum('hvk,hk->hv', recurrent_state, -normed_now, precision=lax.Precision.HIGHEST)
        recurrent_state = recurrent_state * jnp.exp(logdec_now)[:, None, :] + recall[:, :, None] * (normed_now * learn_now)[:, None, :] + value_now[:, :, None] * key_now[:, None, :]
        return (recurrent_state, jnp.einsum('hvk,hk->hv', recurrent_state, query_now, precision=lax.Precision.HIGHEST))
    start = jnp.zeros((number_heads, head_dimension_size, head_dimension_size), jnp.float32)
    _, head_shaped = lax.scan(advance, start, (query_matrix, key_matrix, value_matrix, normalized, learning_rate, log_decay))
    return head_result(head_shaped, query_matrix, key_matrix, value_matrix, output_gate, head_norm_gain, self_weight, head_dimension_size)

def reference(stream, query_first, key_first, value_first, decay_first, learning_first, output_gate_first, extra_decay_first, head_norm_gain_first, self_weight_first, query_second, key_second, value_second, decay_second, learning_second, output_gate_second, extra_decay_second, head_norm_gain_second, self_weight_second, output_projection_first, output_projection_second, middle_norm_gain, mixer_up_weight, mixer_down_weight, final_norm_gain):
    first_mixer = apply_group(query_first, key_first, value_first, decay_first, learning_first, extra_decay_first, output_gate_first, head_norm_gain_first, self_weight_first, FIRST_HEAD_SIZE)
    second_mixer = apply_group(query_second, key_second, value_second, decay_second, learning_second, extra_decay_second, output_gate_second, head_norm_gain_second, self_weight_second, SECOND_HEAD_SIZE)
    mixed = jnp.dot(first_mixer, output_projection_first, preferred_element_type=jnp.float32) + jnp.dot(second_mixer, output_projection_second, preferred_element_type=jnp.float32)
    middle = normalize(ALPHA * stream.astype(jnp.float32) + mixed, middle_norm_gain).astype(jnp.bfloat16)
    hidden = jnp.square(jax.nn.relu(jnp.dot(middle, mixer_up_weight, preferred_element_type=jnp.float32))).astype(jnp.bfloat16)
    block_width = FF // N_TP
    ff_total = jnp.zeros((middle.shape[0], D), jnp.float32)
    for part_index in range(N_TP):
        lower_edge = part_index * block_width
        partial_sum = jnp.dot(hidden[:, lower_edge:lower_edge + block_width], mixer_down_weight[lower_edge:lower_edge + block_width], preferred_element_type=jnp.float32).astype(jnp.bfloat16)
        partial_sum = lax.optimization_barrier(partial_sum)
        ff_total = ff_total + partial_sum.astype(jnp.float32)
    return normalize(ALPHA * middle.astype(jnp.float32) + ff_total, final_norm_gain).astype(jnp.bfloat16)
```

```python
import jax
import jax.numpy as jnp
from jax import lax
from jax.experimental import pallas as pl
from jax.experimental.pallas import tpu as pltpu
from jax.sharding import Mesh
from jax.sharding import PartitionSpec as P

CHUNK = 64
LANES = 128
FIRST_HEAD_SIZE = 64
SECOND_HEAD_SIZE = 128
SP = ("z", "y")
TP = ("x", "c")
ALL = ("z", "y", "x", "c")
EPS_KEY = 1e-05
EPS_HEAD = 0.00064
EPS_NORM = 1e-05
ALPHA = 2.0**0.25
F32 = jnp.float32
BF16 = jnp.bfloat16


def mm(a, b):
    return jnp.dot(a.astype(BF16), b.astype(BF16), preferred_element_type=F32)


def mm_nt(a, b):
    return lax.dot_general(
        a.astype(BF16), b.astype(BF16), (((1,), (1,)), ((), ())), preferred_element_type=F32
    )


def mm_tn(a, b):
    return lax.dot_general(
        a.astype(BF16), b.astype(BF16), (((0,), (0,)), ((), ())), preferred_element_type=F32
    )


def iotas(rows=LANES, cols=LANES):
    return (
        lax.broadcasted_iota(jnp.int32, (rows, cols), 0),
        lax.broadcasted_iota(jnp.int32, (rows, cols), 1),
    )


def halves(rows):
    return lax.broadcasted_iota(jnp.int32, (rows, LANES), 1) < FIRST_HEAD_SIZE


def head_mean(array, pair):
    if not pair:
        return jnp.mean(array, -1, keepdims=True)
    low = halves(array.shape[0])
    first = jnp.sum(jnp.where(low, array, 0.0), -1, keepdims=True)
    second = jnp.sum(jnp.where(low, 0.0, array), -1, keepdims=True)
    return jnp.where(low, first, second) / FIRST_HEAD_SIZE


def spread(array):
    low = halves(array.shape[0])
    return jnp.concatenate([jnp.where(low, array, 0.0), jnp.where(low, 0.0, array)], 0)


def features(q_ref, k_ref, v_ref, d_ref, l_ref, e_ref, pair):
    q, k, v = (r[...].astype(F32) for r in (q_ref, k_ref, v_ref))
    size = FIRST_HEAD_SIZE if pair else SECOND_HEAD_SIZE
    normed = k * lax.rsqrt(head_mean(k * k, pair) + EPS_KEY) * size ** (-0.5)
    learn = jax.nn.sigmoid(l_ref[...].astype(F32))
    burst = e_ref[...]
    if pair:
        burst = jnp.where(halves(q.shape[0]), burst[:, 0:1], burst[:, 1:2])
    logdec = jax.nn.sigmoid(d_ref[...].astype(F32)) * (-(2.718281828459045**-0.5)) + burst
    return q, k, v, normed, learn, logdec


def running_sum(logdec):
    rows, cols = iotas()
    tri = ((rows // CHUNK == cols // CHUNK) & (cols <= rows)).astype(BF16)
    high = logdec.astype(BF16)
    rest = logdec - high.astype(F32)
    mid = rest.astype(BF16)
    low = (rest - mid.astype(F32)).astype(BF16)
    return mm(tri, high) + (mm(tri, mid) + mm(tri, low))


def chunk_row(array, at):
    return jnp.concatenate(
        [
            jnp.broadcast_to(array[c * CHUNK + at : c * CHUNK + at + 1], (CHUNK, array.shape[1]))
            for c in range(array.shape[0] // CHUNK)
        ],
        0,
    )


def inverses(lowers):
    rows, cols = iotas()
    eye = (rows == cols).astype(F32)
    found = [eye + jnp.where(rows // 2 == cols // 2, low, 0.0) for low in lowers]
    step = 2
    while step < CHUNK:
        mask = (rows // (2 * step) == cols // (2 * step)) & (rows // step != cols // step)
        short = [x.astype(BF16) for x in found]
        part = [mm(x, jnp.where(mask, low, 0.0)) for x, low in zip(short, lowers)]
        found = [f + mm(p, x) for f, p, x in zip(found, part, short)]
        step *= 2
    return found


def maps_kernel(*refs):
    ins, outs, carry = refs[:12], refs[12:21], refs[21]
    step = pl.program_id(0)
    rows, cols = iotas()
    same = rows // CHUNK == cols // CHUNK
    strict = same & (cols < rows)
    inclusive = same & (cols <= rows)
    eye = (rows == cols).astype(F32)

    @pl.when(step == 0)
    def _():
        for g in range(2):
            carry[g, :LANES, :] = eye
            carry[g, LANES:, :] = jnp.zeros((LANES, LANES), F32)

    units = []
    keeps = []
    for g in range(2):
        q, k, v, normed, learn, logdec = features(*ins[6 * g : 6 * g + 6], g == 0)
        forward, backward = -normed, normed * learn
        cumul = running_sum(logdec)
        before = cumul - logdec
        middle = chunk_row(cumul, CHUNK // 2)
        ending = chunk_row(cumul, CHUNK - 1)
        up, down, left = jnp.exp(before - middle), jnp.exp(middle - cumul), jnp.exp(ending - cumul)
        keeps.append([jnp.exp(cumul[c * CHUNK + CHUNK - 1 : (c + 1) * CHUNK]) for c in range(2)])
        parts = (
            forward * up,
            q * jnp.exp(cumul - middle),
            backward * down,
            k * down,
            forward * jnp.exp(before),
            q * jnp.exp(cumul),
            backward * left,
            k * left,
            v,
        )
        if g == 0:
            for c in range(2):
                units.append([spread(p[c * CHUNK : (c + 1) * CHUNK]) for p in parts])
        else:
            units.append(list(parts))
    units = [[p.astype(BF16) for p in u[:5]] + [u[5]] + [p.astype(BF16) for p in u[6:]] for u in units]
    grams = [
        mm_nt(jnp.concatenate([u[0], u[1]], 0), jnp.concatenate([u[2], u[3]], 0)) for u in units
    ]
    lowers = [jnp.where(strict, m[:LANES, :LANES], 0.0) for m in grams]
    writes = [jnp.where(strict, m[:LANES, LANES:], 0.0) for m in grams]
    read_corr = [jnp.where(inclusive, m[LANES:, :LANES], 0.0) for m in grams]
    read_write = [jnp.where(inclusive, m[LANES:, LANES:], 0.0) for m in grams]
    solvers = inverses(lowers)
    sides = [
        jnp.concatenate([u[4], mm(w, u[8]).astype(BF16)], 1) for u, w in zip(units, writes)
    ]
    solved = [mm(x, s).astype(BF16) for x, s in zip(solvers, sides)]
    carried = [mm(r, s) for r, s in zip(read_corr, solved)]
    entry = [u[5] + c[:, :LANES] for u, c in zip(units, carried)]
    inner = [c[:, LANES:] + mm(r, u[8]) for u, c, r in zip(units, carried, read_write)]
    moved = []
    for n, (u, s) in enumerate(zip(units, solved)):
        for c in range(1 if n < 2 else 2):
            at = slice(0, LANES) if n < 2 else slice(c * CHUNK, (c + 1) * CHUNK)
            both = mm_tn(s[at], u[6][at])
            moved.append((both[:LANES], both[LANES:] + mm_tn(u[8][at], u[7][at])))
    entry_1, inner_1, entry_2, inner_2, starts_q1, starts_z1, starts_q2, starts_z2, total = outs
    for c in range(2):
        at = slice(c * CHUNK, (c + 1) * CHUNK)
        entry_1[at] = (entry[c][:CHUNK] + entry[c][CHUNK:]).astype(BF16)
        inner_1[at] = inner[c][:CHUNK] + inner[c][CHUNK:]
    entry_2[...] = entry[2].astype(BF16)
    inner_2[...] = inner[2]
    held = [carry[0], carry[1]]
    for c in range(2):
        for g, (sq, sz) in enumerate(((starts_q1, starts_z1), (starts_q2, starts_z2))):
            sq[c] = held[g][:LANES].astype(BF16)
            sz[c] = held[g][LANES:]
            transit, update = moved[2 * g + c]
            after = held[g] * keeps[g][c] + mm(held[g], transit)
            held[g] = jnp.concatenate([after[:LANES], after[LANES:] + update], 0)
    for g in range(2):
        carry[g] = held[g]

    @pl.when(step == pl.num_programs(0) - 1)
    def _():
        first, second = held
        total[0:64] = (first[0:64] + first[64:128]).astype(BF16)
        total[64:128] = (first[128:192] + first[192:256]).astype(BF16)
        total[128:384] = second.astype(BF16)


def chunk_maps(first, second):
    tokens = first[0].shape[0]
    steps = tokens // LANES
    chunks = tokens // CHUNK

    def rows(width=LANES):
        return pl.BlockSpec((LANES, width), lambda i: (i, 0))

    state = pl.BlockSpec((2, LANES, LANES), lambda i: (i, 0, 0))
    ins = []
    for group in (first, second):
        ins += [rows()] * 5 + [rows(group[5].shape[1])]
    return pl.pallas_call(
        maps_kernel,
        grid=(steps,),
        in_specs=ins,
        out_specs=[rows()] * 4 + [state] * 4 + [pl.BlockSpec((384, LANES), lambda i: (0, 0))],
        out_shape=[
            jax.ShapeDtypeStruct((tokens, LANES), t) for t in (BF16, F32, BF16, F32)
        ]
        + [jax.ShapeDtypeStruct((chunks, LANES, LANES), t) for t in (BF16, F32, BF16, F32)]
        + [jax.ShapeDtypeStruct((384, LANES), BF16)],
        scratch_shapes=[pltpu.VMEM((2, 2 * LANES, LANES), F32)],
        cost_estimate=pl.CostEstimate(
            flops=12_000_000_000, bytes_accessed=8_000_000, transcendentals=2_000_000
        ),
        name="chunk_maps",
    )(*first, *second)


def unpack(packed):
    def widen(part):
        return spread(part.astype(F32))

    return (
        jnp.concatenate([widen(packed[0:64]), widen(packed[64:128])], 0),
        packed[128:384].astype(F32),
    )


def pack(pairs):
    first, second = pairs
    return jnp.concatenate(
        [first[0:64] + first[64:128], first[128:192] + first[192:256], second], 0
    )


def compose(earlier, later):
    out = []
    for a, b in zip(earlier, later):
        moved = mm(a, b[:LANES])
        out.append(jnp.concatenate([moved[:LANES], moved[LANES:] + b[LANES:]], 0))
    return out


def row_kernel(mine_ref, own, one, two, three, before_ref, total_ref):
    mine = mine_ref[0]
    by_shift = [r[...] for r in (own, one, two, three)]

    def member(k):
        shift = lax.rem(mine - k + 4, 4)
        out = by_shift[3]
        for s in range(3):
            out = jnp.where(shift == s, by_shift[s], out)
        return unpack(out)

    rows, cols = iotas()
    eye = (rows == cols).astype(F32)
    neutral = jnp.concatenate([eye, jnp.zeros((LANES, LANES), F32)], 0)
    running = member(0)
    before = [jnp.where(mine == 0, neutral, r) for r in running]
    for k in range(1, 4):
        before = [jnp.where(mine == k, r, b) for r, b in zip(running, before)] if k > 1 else [
            jnp.where(mine == 0, neutral, r) for r in running
        ]
        running = compose(running, member(k))
    before_ref[...] = pack(before)
    total_ref[...] = pack(running)


def vmem_call(kernel, out_shape, *args, scalars=0, name=None):
    return pl.pallas_call(
        kernel,
        in_specs=[pl.BlockSpec(memory_space=pltpu.SMEM)] * scalars
        + [pl.BlockSpec(memory_space=pltpu.VMEM)] * (len(args) - scalars),
        out_specs=jax.tree.map(lambda _: pl.BlockSpec(memory_space=pltpu.VMEM), out_shape),
        out_shape=out_shape,
        name=name,
    )(*args)


def join_kernel(earlier_ref, later_ref, out_ref):
    out_ref[...] = pack(compose(unpack(earlier_ref[...]), unpack(later_ref[...])))


def join_two_kernel(earlier_ref, before_ref, through_ref, before_out, through_out):
    earlier = unpack(earlier_ref[...])
    before_out[...] = pack(compose(earlier, unpack(before_ref[...])))
    through_out[...] = pack(compose(earlier, unpack(through_ref[...])))


def shift(array, axis, by, size, wrap):
    pairs = [(i, (i + by) % size) for i in range(size) if wrap or 0 <= i + by < size]
    return lax.ppermute(array, axis, pairs)


def sequence_prefix(total):
    shape = jax.ShapeDtypeStruct(total.shape, F32)
    ny, nz = lax.axis_size("y"), lax.axis_size("z")
    peers = [shift(total, "y", s, ny, True) for s in (1, 2, 3)]
    mine = lax.axis_index("y").astype(jnp.int32).reshape(1)
    row_before, row_total = vmem_call(
        row_kernel, (shape, shape), mine, total, *peers, scalars=1, name="row_maps"
    )
    before = shift(row_total.astype(BF16), "z", 1, nz, False)
    through = vmem_call(join_kernel, shape, before, row_total, name="join_one")
    earlier = shift(through.astype(BF16), "z", 2, nz, False)
    before, through = vmem_call(
        join_two_kernel, (shape, shape), earlier, before, through, name="join_two"
    )
    send = jnp.concatenate([through[64:128], through[256:384]], 0).astype(BF16)
    last = shift(send, "z", 4, nz, False)
    return last, before, row_before


def outputs_kernel(*refs):
    (last, before, row_before), ins, out, states = refs[:3], refs[3:19], refs[19], refs[20]

    @pl.when(pl.program_id(0) == 0)
    def _():
        near = unpack(before[...])
        row = unpack(row_before[...])
        far = (spread(last[0:64].astype(F32)), last[64:192])
        for g in range(2):
            start = mm(far[g], near[g][:LANES]) + near[g][LANES:]
            states[g] = mm(start, row[g][:LANES]) + row[g][LANES:]

    for g in range(2):
        entry, inner, sq, sz, q_ref, k_ref, v_ref, gate_ref = ins[8 * g : 8 * g + 8]
        pair = g == 0
        gain, weight = out_params(refs, g)
        start = states[g].astype(BF16)
        pieces = []
        for c in range(2):
            at = slice(c * CHUNK, (c + 1) * CHUNK)
            state = mm(start, sq[c]) + sz[c]
            pieces.append(mm_nt(entry[at], state) + inner[at])
        heady = jnp.concatenate(pieces, 0)
        q, k, v, gate = (r[...].astype(F32) for r in (q_ref, k_ref, v_ref, gate_ref))
        centred = heady - head_mean(heady, pair)
        spread_ = head_mean(centred * centred, pair)
        normalized = centred * lax.rsqrt(spread_ + EPS_HEAD) * gain
        size = FIRST_HEAD_SIZE if pair else SECOND_HEAD_SIZE
        extra = head_mean(q * k * weight, pair) * size * v
        out[:, g * LANES : (g + 1) * LANES] = (
            (normalized + extra) * jax.nn.sigmoid(gate)
        ).astype(BF16)


def out_params(refs, g):
    params = refs[21]
    return params[2 * g : 2 * g + 1], params[2 * g + 1 : 2 * g + 2]


def mixer_outputs(prefix, groups, params):
    tokens = groups[0][0].shape[0]
    rows = pl.BlockSpec((LANES, LANES), lambda i: (i, 0))
    state = pl.BlockSpec((2, LANES, LANES), lambda i: (i, 0, 0))

    def whole(a):
        return pl.BlockSpec(a.shape, lambda i: (0,) * a.ndim)

    def kernel(*refs):
        ins, out, states = refs[:20], refs[20], refs[21]
        outputs_kernel(*ins[:19], out, states, ins[19])

    return pl.pallas_call(
        kernel,
        grid=(tokens // LANES,),
        in_specs=[whole(a) for a in prefix]
        + [rows, rows, state, state, rows, rows, rows, rows] * 2
        + [whole(params)],
        out_specs=pl.BlockSpec((LANES, 2 * LANES), lambda i: (i, 0)),
        out_shape=jax.ShapeDtypeStruct((tokens, 2 * LANES), BF16),
        scratch_shapes=[pltpu.VMEM((2, LANES, LANES), F32)],
        cost_estimate=pl.CostEstimate(
            flops=2_000_000_000, bytes_accessed=6_000_000, transcendentals=300_000
        ),
        name="mixer_outputs",
    )(*prefix, *groups[0], *groups[1], params)


def norm_rows(array, gain):
    mean_part = jnp.mean(array, -1, keepdims=True)
    centred = array - mean_part
    return centred * lax.rsqrt(jnp.mean(centred * centred, -1, keepdims=True) + EPS_NORM) * gain


def project_kernel(rows_ref, first_ref, second_ref, stream_ref, gain_ref, out_ref, acc):
    step = pl.program_id(0)
    rows = rows_ref[0]

    @pl.when(step == 0)
    def _():
        acc[...] = ALPHA * stream_ref[...].astype(F32)

    acc[...] += jnp.dot(rows[:, :LANES], first_ref[...], preferred_element_type=F32) + jnp.dot(
        rows[:, LANES:], second_ref[...], preferred_element_type=F32
    )

    @pl.when(step == pl.num_programs(0) - 1)
    def _():
        out_ref[...] = norm_rows(acc[...], gain_ref[...]).astype(BF16)


def project(rows, first, second, stream, gain):
    peers, count, _ = rows.shape
    width = first.shape[1]
    weight = pl.BlockSpec((LANES, width), lambda i: (i, 0))
    return pl.pallas_call(
        project_kernel,
        grid=(peers,),
        in_specs=[
            pl.BlockSpec((1, count, 2 * LANES), lambda i: (i, 0, 0)),
            weight,
            weight,
            pl.BlockSpec((count, width), lambda i: (0, 0)),
            pl.BlockSpec((1, width), lambda i: (0, 0)),
        ],
        out_specs=pl.BlockSpec((count, width), lambda i: (0, 0)),
        out_shape=jax.ShapeDtypeStruct((count, width), BF16),
        scratch_shapes=[pltpu.VMEM((count, width), F32)],
        cost_estimate=pl.CostEstimate(
            flops=4_000_000_000, bytes_accessed=9_000_000, transcendentals=100
        ),
        name="project",
    )(rows, first, second, stream, gain.reshape(1, -1))


def swap_core(array):
    return lax.ppermute(array, "c", [(0, 1), (1, 0)])


def local(
    stream,
    query_first,
    key_first,
    value_first,
    decay_first,
    learning_first,
    output_gate_first,
    extra_decay_first,
    head_norm_gain_first,
    self_weight_first,
    query_second,
    key_second,
    value_second,
    decay_second,
    learning_second,
    output_gate_second,
    extra_decay_second,
    head_norm_gain_second,
    self_weight_second,
    output_projection_first,
    output_projection_second,
    middle_norm_gain,
    mixer_up_weight,
    mixer_down_weight,
    final_norm_gain,
):
    count, width = stream.shape
    depth = mixer_up_weight.shape[0]
    hidden_width = mixer_up_weight.shape[1]
    both = jnp.concatenate([mixer_up_weight, mixer_down_weight.T], 0)
    weights = lax.all_gather(both, SP)
    up_whole = weights[:, :depth].reshape(-1, hidden_width)
    down_whole = weights[:, depth:].reshape(-1, hidden_width)

    maps = chunk_maps(
        (query_first, key_first, value_first, decay_first, learning_first, extra_decay_first),
        (query_second, key_second, value_second, decay_second, learning_second, extra_decay_second),
    )
    entry_1, inner_1, entry_2, inner_2, sq1, sz1, sq2, sz2, total = maps
    prefix = sequence_prefix(total)
    params = jnp.stack(
        [head_norm_gain_first, self_weight_first, head_norm_gain_second, self_weight_second]
    )
    mixer = mixer_outputs(
        prefix,
        (
            (entry_1, inner_1, sq1, sz1, query_first, key_first, value_first, output_gate_first),
            (entry_2, inner_2, sq2, sz2, query_second, key_second, value_second, output_gate_second),
        ),
        params,
    )
    rows = lax.all_to_all(mixer.reshape(-1, count, 2 * LANES), TP, 0, 0, tiled=True)
    middle = project(
        rows, output_projection_first, output_projection_second, stream, middle_norm_gain
    )

    nx = lax.axis_size("x")
    half = count // 2
    near_p = shift(middle, "x", 1, nx, True)
    near_m = shift(middle, "x", -1, nx, True)
    far_p = shift(near_p[:half], "x", 1, nx, True)
    far_m = shift(near_m[half:], "x", -1, nx, True)
    far = jnp.concatenate([far_p, far_m], 0)

    def channel(block):
        rows_all = jnp.concatenate([block, swap_core(block)], 0)
        upward = jnp.dot(rows_all, up_whole, preferred_element_type=F32)
        hidden = jnp.square(jax.nn.relu(upward)).astype(BF16)
        part = lax.dot_general(
            hidden, down_whole, (((1,), (1,)), ((), ())), preferred_element_type=F32
        ).astype(BF16)
        size = block.shape[0]
        return part[:size].astype(F32) + swap_core(part[size:]).astype(F32)

    sum_own = channel(middle)
    sum_near = channel(jnp.concatenate([near_p, near_m], 0))
    sum_far = channel(far)
    sum_p, sum_m = sum_near[:count], sum_near[count:]
    from_p = shift(sum_far[:half].astype(BF16), "x", 1, nx, True).astype(F32)
    from_m = shift(sum_far[half:].astype(BF16), "x", -1, nx, True).astype(F32)
    sum_m = jnp.concatenate([sum_m[:half] + from_p, sum_m[half:]], 0).astype(BF16)
    sum_p = jnp.concatenate([sum_p[:half], sum_p[half:] + from_m], 0).astype(BF16)
    ff_total = (
        sum_own
        + shift(sum_p, "x", -1, nx, True).astype(F32)
        + shift(sum_m, "x", 1, nx, True).astype(F32)
    )
    return norm_rows(ALPHA * middle.astype(F32) + ff_total, final_norm_gain).astype(BF16)


def solution(mesh):
    split = Mesh(mesh.devices.reshape(8, 4, 4, 2), ALL)
    long = P(SP, TP)
    group = (long,) * 7 + (P(TP), P(TP))
    return jax.shard_map(
        local,
        mesh=split,
        in_specs=(P(ALL, None),)
        + group
        + group
        + (P(), P(), P(), P(SP, TP), P(TP, SP), P()),
        out_specs=P(ALL, None),
        check_vma=False,
    )
```

```python
import jax
import jax.numpy as jnp
from jax import lax
from jax.experimental import pallas as pl
from jax.experimental.pallas import tpu as pltpu
from jax.sharding import Mesh
from jax.sharding import PartitionSpec as P

CHUNK = 64
LANES = 128
FIRST_HEAD_SIZE = 64
SECOND_HEAD_SIZE = 128
SP = ("z", "y")
TP = ("x", "c")
ALL = ("z", "y", "x", "c")
EPS_KEY = 1e-05
EPS_HEAD = 0.00064
EPS_NORM = 1e-05
ALPHA = 2.0**0.25
F32 = jnp.float32
BF16 = jnp.bfloat16


def mm(a, b):
    return jnp.dot(a.astype(BF16), b.astype(BF16), preferred_element_type=F32)


def mm_nt(a, b):
    return lax.dot_general(
        a.astype(BF16), b.astype(BF16), (((1,), (1,)), ((), ())), preferred_element_type=F32
    )


def mm_tn(a, b):
    return lax.dot_general(
        a.astype(BF16), b.astype(BF16), (((0,), (0,)), ((), ())), preferred_element_type=F32
    )


def iotas(rows=LANES, cols=LANES):
    return (
        lax.broadcasted_iota(jnp.int32, (rows, cols), 0),
        lax.broadcasted_iota(jnp.int32, (rows, cols), 1),
    )


def halves(rows):
    return lax.broadcasted_iota(jnp.int32, (rows, LANES), 1) < FIRST_HEAD_SIZE


def head_mean(array, pair):
    if not pair:
        return jnp.mean(array, -1, keepdims=True)
    low = halves(array.shape[0])
    first = jnp.sum(jnp.where(low, array, 0.0), -1, keepdims=True)
    second = jnp.sum(jnp.where(low, 0.0, array), -1, keepdims=True)
    return jnp.where(low, first, second) / FIRST_HEAD_SIZE


def spread(array):
    low = halves(array.shape[0])
    return jnp.concatenate([jnp.where(low, array, 0.0), jnp.where(low, 0.0, array)], 0)


def features(q_ref, k_ref, v_ref, d_ref, l_ref, e_ref, pair):
    q, k, v = (r[...].astype(F32) for r in (q_ref, k_ref, v_ref))
    size = FIRST_HEAD_SIZE if pair else SECOND_HEAD_SIZE
    normed = k * lax.rsqrt(head_mean(k * k, pair) + EPS_KEY) * size ** (-0.5)
    learn = jax.nn.sigmoid(l_ref[...].astype(F32))
    heads = e_ref.shape[0]
    rows, cols = iotas(heads, LANES)
    owner = (cols // size == rows).astype(BF16)
    burst = sum(mm_tn(part, owner) for part in split3(e_ref[...]))
    logdec = jax.nn.sigmoid(d_ref[...].astype(F32)) * (-(2.718281828459045**-0.5)) + burst
    return q, k, v, normed, learn, logdec


def split3(array):
    high = array.astype(BF16)
    rest = array - high.astype(F32)
    mid = rest.astype(BF16)
    return high, mid, (rest - mid.astype(F32)).astype(BF16)


def running_sum(logdec):
    rows, cols = iotas()
    tri = ((rows // CHUNK == cols // CHUNK) & (cols <= rows)).astype(BF16)
    return jnp.concatenate(
        [
            sum(mm(tri, part) for part in split3(logdec[at : at + LANES]))
            for at in range(0, logdec.shape[0], LANES)
        ],
        0,
    )


def chunk_row(array, at):
    return jnp.concatenate(
        [
            jnp.broadcast_to(array[c * CHUNK + at : c * CHUNK + at + 1], (CHUNK, array.shape[1]))
            for c in range(array.shape[0] // CHUNK)
        ],
        0,
    )


def inverses(lowers):
    rows, cols = iotas()
    eye = (rows == cols).astype(F32)
    found = [eye + jnp.where(rows // 2 == cols // 2, low, 0.0) for low in lowers]
    step = 2
    while step < CHUNK:
        mask = (rows // (2 * step) == cols // (2 * step)) & (rows // step != cols // step)
        short = [x.astype(BF16) for x in found]
        part = [mm(x, jnp.where(mask, low, 0.0)) for x, low in zip(short, lowers)]
        found = [f + mm(p, x) for f, p, x in zip(found, part, short)]
        step *= 2
    return found


def maps_kernel(*refs):
    ins, outs, carry = refs[:12], refs[12:21], refs[21]
    solved_ref, reads_ref, begin_1, begin_2, starts_q1, starts_z1, starts_q2, starts_z2, total = outs
    tokens = begin_1.shape[0]
    blocks, chunks = tokens // LANES, tokens // CHUNK
    step = pl.program_id(0)
    rows, cols = iotas()
    same = rows // CHUNK == cols // CHUNK
    strict = same & (cols < rows)
    inclusive = same & (cols <= rows)

    @pl.when(step == 0)
    def _():
        for g in range(2):
            carry[g, :LANES, :] = (rows == cols).astype(F32)
            carry[g, LANES:, :] = jnp.zeros((LANES, LANES), F32)

    units = [None] * (3 * blocks)
    keeps = []
    for g in range(2):
        q, k, v, normed, learn, logdec = features(*ins[6 * g : 6 * g + 6], g == 0)
        forward, backward = -normed, normed * learn
        cumul = running_sum(logdec)
        before = cumul - logdec
        middle = chunk_row(cumul, CHUNK // 2)
        ending = chunk_row(cumul, CHUNK - 1)
        up, down, left = jnp.exp(before - middle), jnp.exp(middle - cumul), jnp.exp(ending - cumul)
        keeps.append(
            [jnp.exp(cumul[(c + 1) * CHUNK - 1 : (c + 1) * CHUNK]) for c in range(chunks)]
        )
        (begin_1, begin_2)[g][...] = (q * jnp.exp(cumul)).astype(BF16)
        parts = (
            forward * up,
            q * jnp.exp(cumul - middle),
            backward * down,
            k * down,
            forward * jnp.exp(before),
            backward * left,
            k * left,
            v,
        )
        for b in range(blocks):
            if g == 0:
                for c in range(2):
                    at = b * LANES + c * CHUNK
                    units[3 * b + c] = [spread(p[at : at + CHUNK]).astype(BF16) for p in parts]
            else:
                units[3 * b + 2] = [p[b * LANES : (b + 1) * LANES].astype(BF16) for p in parts]
    grams = [
        mm_nt(jnp.concatenate([u[0], u[1]], 0), jnp.concatenate([u[2], u[3]], 0)) for u in units
    ]
    lowers = [jnp.where(strict, m[:LANES, :LANES], 0.0) for m in grams]
    writes = [jnp.where(strict, m[:LANES, LANES:], 0.0) for m in grams]
    for n, m in enumerate(grams):
        reads_ref[n, :, :LANES] = jnp.where(inclusive, m[LANES:, :LANES], 0.0).astype(BF16)
        reads_ref[n, :, LANES:] = jnp.where(inclusive, m[LANES:, LANES:], 0.0).astype(BF16)
    solvers = inverses(lowers)
    sides = [
        jnp.concatenate([u[4], mm(w, u[7]).astype(BF16)], 1) for u, w in zip(units, writes)
    ]
    solved = [mm(x, s).astype(BF16) for x, s in zip(solvers, sides)]
    moved = [[], []]
    for n, (u, s) in enumerate(zip(units, solved)):
        solved_ref[n] = s
        g = int(n % 3 == 2)
        for c in range(1 + g):
            at = slice(c * CHUNK, (c + 1) * CHUNK) if g else slice(0, LANES)
            both = mm_tn(s[at], u[5][at])
            moved[g].append((both[:LANES], both[LANES:] + mm_tn(u[7][at], u[6][at])))
    held = [carry[0], carry[1]]
    for c in range(chunks):
        for g, (sq, sz) in enumerate(((starts_q1, starts_z1), (starts_q2, starts_z2))):
            sq[c] = held[g][:LANES].astype(BF16)
            sz[c] = held[g][LANES:]
            transit, update = moved[g][c]
            after = held[g] * keeps[g][c] + mm(held[g], transit)
            held[g] = jnp.concatenate([after[:LANES], after[LANES:] + update], 0)
    for g in range(2):
        carry[g] = held[g]

    @pl.when(step == pl.num_programs(0) - 1)
    def _():
        total[...] = pack(held)


def chunk_maps(first, second):
    tokens = first[0].shape[0]
    block = 256
    chunks = tokens // CHUNK
    units = 3 * tokens // LANES
    rows = pl.BlockSpec((block, LANES), lambda i: (i, 0))
    state = pl.BlockSpec((block // CHUNK, LANES, LANES), lambda i: (i, 0, 0))
    unit = pl.BlockSpec((3 * block // LANES, LANES, 2 * LANES), lambda i: (i, 0, 0))
    ins = []
    for group in (first, second):
        ins += [rows] * 5 + [pl.BlockSpec((group[5].shape[0], block), lambda i: (0, i))]
    return pl.pallas_call(
        maps_kernel,
        grid=(tokens // block,),
        in_specs=ins,
        out_specs=[unit] * 2
        + [rows] * 2
        + [state] * 4
        + [pl.BlockSpec((384, LANES), lambda i: (0, 0))],
        out_shape=[jax.ShapeDtypeStruct((units, LANES, 2 * LANES), BF16)] * 2
        + [jax.ShapeDtypeStruct((tokens, LANES), BF16)] * 2
        + [jax.ShapeDtypeStruct((chunks, LANES, LANES), t) for t in (BF16, F32, BF16, F32)]
        + [jax.ShapeDtypeStruct((384, LANES), BF16)],
        scratch_shapes=[pltpu.VMEM((2, 2 * LANES, LANES), F32)],
        cost_estimate=pl.CostEstimate(
            flops=12_000_000_000, bytes_accessed=8_000_000, transcendentals=2_000_000
        ),
        name="chunk_maps",
    )(*first, *second)


def reads_kernel(solved, reads, begin_1, begin_2, v_1, v_2, entry_1, inner_1, entry_2, inner_2):
    for b in range(begin_1.shape[0] // LANES):
        for u in range(3):
            n = 3 * b + u
            at = slice(b * LANES + u * CHUNK, b * LANES + (u + 1) * CHUNK)
            if u == 2:
                at = slice(b * LANES, (b + 1) * LANES)
            value = v_2[at] if u == 2 else spread(v_1[at].astype(F32)).astype(BF16)
            carried = mm(reads[n, :, :LANES], solved[n])
            entry = carried[:, :LANES]
            inner = carried[:, LANES:] + mm(reads[n, :, LANES:], value)
            if u == 2:
                entry_2[at] = (begin_2[at].astype(F32) + entry).astype(BF16)
                inner_2[at] = inner
            else:
                entry_1[at] = (begin_1[at].astype(F32) + entry[:CHUNK] + entry[CHUNK:]).astype(BF16)
                inner_1[at] = inner[:CHUNK] + inner[CHUNK:]


def chunk_reads(solved, reads, begin_1, begin_2, v_1, v_2):
    tokens = begin_1.shape[0]
    block = 256
    rows = pl.BlockSpec((block, LANES), lambda i: (i, 0))
    unit = pl.BlockSpec((3 * block // LANES, LANES, 2 * LANES), lambda i: (i, 0, 0))
    return pl.pallas_call(
        reads_kernel,
        grid=(tokens // block,),
        in_specs=[unit, unit] + [rows] * 4,
        out_specs=[rows] * 4,
        out_shape=[jax.ShapeDtypeStruct((tokens, LANES), t) for t in (BF16, F32, BF16, F32)],
        cost_estimate=pl.CostEstimate(
            flops=4_000_000_000, bytes_accessed=6_000_000, transcendentals=0
        ),
        name="chunk_reads",
    )(solved, reads, begin_1, begin_2, v_1, v_2)


def unpack(packed):
    def widen(part):
        return spread(part.astype(F32))

    return (
        jnp.concatenate([widen(packed[0:64]), widen(packed[64:128])], 0),
        packed[128:384].astype(F32),
    )


def pack(pairs):
    first, second = pairs
    return jnp.concatenate(
        [first[0:64] + first[64:128], first[128:192] + first[192:256], second], 0
    ).astype(BF16)


def compose(earlier, later):
    out = []
    for a, b in zip(earlier, later):
        moved = mm(a, b[:LANES])
        out.append(jnp.concatenate([moved[:LANES], moved[LANES:] + b[LANES:]], 0))
    return out


def row_kernel(mine_ref, own, one, two, three, before_ref, total_ref):
    mine = mine_ref[0]
    by_shift = [r[...] for r in (own, one, two, three)]

    def member(k):
        shift = lax.rem(mine - k + 4, 4)
        out = by_shift[3]
        for s in range(3):
            out = jnp.where(shift == s, by_shift[s], out)
        return unpack(out)

    rows, cols = iotas()
    eye = (rows == cols).astype(F32)
    neutral = jnp.concatenate([eye, jnp.zeros((LANES, LANES), F32)], 0)
    running = member(0)
    before = [jnp.where(mine == 0, neutral, r) for r in running]
    for k in range(1, 4):
        before = [jnp.where(mine == k, r, b) for r, b in zip(running, before)] if k > 1 else [
            jnp.where(mine == 0, neutral, r) for r in running
        ]
        running = compose(running, member(k))
    before_ref[...] = pack(before)
    total_ref[...] = pack(running)


def vmem_call(kernel, out_shape, *args, scalars=0, name=None):
    return pl.pallas_call(
        kernel,
        in_specs=[pl.BlockSpec(memory_space=pltpu.SMEM)] * scalars
        + [pl.BlockSpec(memory_space=pltpu.VMEM)] * (len(args) - scalars),
        out_specs=jax.tree.map(lambda _: pl.BlockSpec(memory_space=pltpu.VMEM), out_shape),
        out_shape=out_shape,
        name=name,
    )(*args)


def join_kernel(earlier_ref, later_ref, out_ref):
    out_ref[...] = pack(compose(unpack(earlier_ref[...]), unpack(later_ref[...])))


def join_two_kernel(earlier_ref, before_ref, through_ref, before_out, through_out):
    earlier = unpack(earlier_ref[...])
    before_out[...] = pack(compose(earlier, unpack(before_ref[...])))
    through = pack(compose(earlier, unpack(through_ref[...])))
    through_out[0:64] = through[64:128]
    through_out[64:192] = through[256:384]


def shift(array, axis, by, size, wrap):
    pairs = [(i, (i + by) % size) for i in range(size) if wrap or 0 <= i + by < size]
    return lax.ppermute(array, axis, pairs)


def sequence_prefix(total, entries):
    shape = jax.ShapeDtypeStruct(total.shape, BF16)
    ny, nz = lax.axis_size("y"), lax.axis_size("z")
    peers = [shift(total, "y", s, ny, True) for s in (1, 2, 3)]
    peers, entries = lax.optimization_barrier((peers, entries))
    mine = lax.axis_index("y").astype(jnp.int32).reshape(1)
    row_before, row_total = vmem_call(
        row_kernel, (shape, shape), mine, total, *peers, scalars=1, name="row_maps"
    )
    before = shift(row_total, "z", 1, nz, False)
    through = vmem_call(join_kernel, shape, before, row_total, name="join_one")
    earlier = shift(through, "z", 2, nz, False)
    short = jax.ShapeDtypeStruct((192, LANES), BF16)
    before, send = vmem_call(
        join_two_kernel, (shape, short), earlier, before, through, name="join_two"
    )
    last = shift(send, "z", 4, nz, False)
    return (last, before, row_before), entries


def outputs_kernel(*refs):
    (last, before, row_before), ins, out, states = refs[:3], refs[3:19], refs[19], refs[20]

    @pl.when(pl.program_id(0) == 0)
    def _():
        near = unpack(before[...])
        row = unpack(row_before[...])
        far = (spread(last[0:64].astype(F32)), last[64:192])
        for g in range(2):
            start = mm(far[g], near[g][:LANES]) + near[g][LANES:]
            states[g] = mm(start, row[g][:LANES]) + row[g][LANES:]

    for g in range(2):
        entry, inner, sq, sz, q_ref, k_ref, v_ref, gate_ref = ins[8 * g : 8 * g + 8]
        pair = g == 0
        gain, weight = out_params(refs, g)
        start = states[g].astype(BF16)
        pieces = []
        for c in range(sq.shape[0]):
            at = slice(c * CHUNK, (c + 1) * CHUNK)
            state = mm(start, sq[c]) + sz[c]
            pieces.append(mm_nt(entry[at], state) + inner[at])
        heady = jnp.concatenate(pieces, 0)
        q, k, v, gate = (r[...].astype(F32) for r in (q_ref, k_ref, v_ref, gate_ref))
        centred = heady - head_mean(heady, pair)
        spread_ = head_mean(centred * centred, pair)
        normalized = centred * lax.rsqrt(spread_ + EPS_HEAD) * gain
        size = FIRST_HEAD_SIZE if pair else SECOND_HEAD_SIZE
        extra = head_mean(q * k * weight, pair) * size * v
        out[:, g * LANES : (g + 1) * LANES] = (
            (normalized + extra) * jax.nn.sigmoid(gate)
        ).astype(BF16)


def out_params(refs, g):
    params = refs[21]
    return params[2 * g : 2 * g + 1], params[2 * g + 1 : 2 * g + 2]


def mixer_outputs(prefix, groups, params):
    tokens = groups[0][0].shape[0]
    block = 256
    rows = pl.BlockSpec((block, LANES), lambda i: (i, 0))
    state = pl.BlockSpec((block // CHUNK, LANES, LANES), lambda i: (i, 0, 0))

    def whole(a):
        return pl.BlockSpec(a.shape, lambda i: (0,) * a.ndim)

    def kernel(*refs):
        ins, out, states = refs[:20], refs[20], refs[21]
        outputs_kernel(*ins[:19], out, states, ins[19])

    return pl.pallas_call(
        kernel,
        grid=(tokens // block,),
        in_specs=[whole(a) for a in prefix]
        + [rows, rows, state, state, rows, rows, rows, rows] * 2
        + [whole(params)],
        out_specs=pl.BlockSpec((block, 2 * LANES), lambda i: (i, 0)),
        out_shape=jax.ShapeDtypeStruct((tokens, 2 * LANES), BF16),
        scratch_shapes=[pltpu.VMEM((2, LANES, LANES), F32)],
        cost_estimate=pl.CostEstimate(
            flops=2_000_000_000, bytes_accessed=6_000_000, transcendentals=300_000
        ),
        name="mixer_outputs",
    )(*prefix, *groups[0], *groups[1], params)


def norm_rows(array, gain):
    mean_part = jnp.mean(array, -1, keepdims=True)
    centred = array - mean_part
    return centred * lax.rsqrt(jnp.mean(centred * centred, -1, keepdims=True) + EPS_NORM) * gain


def project_kernel(rows_ref, stream_ref, gain_ref, first, second, out_ref, held, sems):
    peers = rows_ref.shape[0]
    copies = []
    for n in range(peers):
        at = pl.ds(n * LANES, LANES)
        for side, source in enumerate((first, second)):
            copies.append(
                pltpu.make_async_copy(
                    source.at[at, :],
                    held.at[n, pl.ds(side * LANES, LANES), :],
                    sems.at[n, side],
                )
            )
    for copy in copies:
        copy.start()
    total = ALPHA * stream_ref[...].astype(F32)
    for n in range(peers):
        copies[2 * n].wait()
        copies[2 * n + 1].wait()
        total += jnp.dot(rows_ref[n], held[n], preferred_element_type=F32)
    out_ref[...] = norm_rows(total, gain_ref[...]).astype(BF16)


def project(rows, first, second, stream, gain):
    peers, count, _ = rows.shape
    width = first.shape[1]
    near = pl.BlockSpec(memory_space=pltpu.VMEM)
    far = pl.BlockSpec(memory_space=pl.ANY)
    return pl.pallas_call(
        project_kernel,
        in_specs=[near, near, near, far, far],
        out_specs=near,
        out_shape=jax.ShapeDtypeStruct((count, width), BF16),
        scratch_shapes=[
            pltpu.VMEM((peers, 2 * LANES, width), BF16),
            pltpu.SemaphoreType.DMA((peers, 2)),
        ],
        cost_estimate=pl.CostEstimate(
            flops=4_000_000_000, bytes_accessed=9_000_000, transcendentals=100
        ),
        name="project",
    )(rows, stream, gain.reshape(1, -1), first, second)


def swap_core(array):
    return lax.ppermute(array, "c", [(0, 1), (1, 0)])


def channel_kernel(mine_ref, theirs_ref, weights, mine_out, theirs_out, rows, acc, held, sems):
    count, width = mine_ref.shape
    pieces, group, depth, _ = held.shape
    half = pieces // 2
    block = group * depth
    copies = []
    for n in range(pieces):
        side = weights.at[
            pl.ds((n % half) * group, group), pl.ds((n // half) * depth, depth), :
        ]
        copies.append(pltpu.make_async_copy(side, held.at[n], sems.at[n]))
    for copy in copies:
        copy.start()
    for n in range(half):
        at = slice(n * block, (n + 1) * block)
        rows[n, :count] = mine_ref[:, at]
        rows[n, count:] = theirs_ref[:, at]
    for n in range(half):
        copies[n].wait()
        part = jnp.dot(rows[n], held[n].reshape(block, -1), preferred_element_type=F32)
        acc[...] = part if n == 0 else acc[...] + part
    hidden = jnp.square(jnp.maximum(acc[...], 0.0)).astype(BF16)
    for n in range(half):
        copies[half + n].wait()
        part = mm_nt(hidden, held[half + n].reshape(block, -1)).astype(BF16)
        at = slice(n * block, (n + 1) * block)
        mine_out[:, at] = part[:count]
        theirs_out[:, at] = part[count:]


def channel(mine, theirs, weights):
    count, width = mine.shape
    peers, depth, hidden = weights.shape
    pieces = 8
    group = 2 * peers // pieces
    rows = pl.BlockSpec(memory_space=pltpu.VMEM)
    return pl.pallas_call(
        channel_kernel,
        in_specs=[rows, rows, pl.BlockSpec(memory_space=pl.ANY)],
        out_specs=[rows, rows],
        out_shape=[jax.ShapeDtypeStruct((count, width), BF16)] * 2,
        scratch_shapes=[
            pltpu.VMEM((pieces // 2, 2 * count, 2 * width // pieces), BF16),
            pltpu.VMEM((2 * count, hidden), F32),
            pltpu.VMEM((pieces, group, depth // 2, hidden), BF16),
            pltpu.SemaphoreType.DMA((pieces,)),
        ],
        cost_estimate=pl.CostEstimate(
            flops=8 * count * width * hidden,
            bytes_accessed=2 * peers * depth * hidden,
            transcendentals=0,
        ),
        name="channel",
    )(mine, theirs, weights)


def local(
    stream,
    query_first,
    key_first,
    value_first,
    decay_first,
    learning_first,
    output_gate_first,
    extra_decay_first,
    head_norm_gain_first,
    self_weight_first,
    query_second,
    key_second,
    value_second,
    decay_second,
    learning_second,
    output_gate_second,
    extra_decay_second,
    head_norm_gain_second,
    self_weight_second,
    output_projection_first,
    output_projection_second,
    middle_norm_gain,
    mixer_up_weight,
    mixer_down_weight,
    final_norm_gain,
):
    count, width = stream.shape
    both = jnp.concatenate([mixer_up_weight, mixer_down_weight.T], 0)
    weights = lax.all_gather(both, SP)

    solved, reads, begin_1, begin_2, sq1, sz1, sq2, sz2, total = chunk_maps(
        (query_first, key_first, value_first, decay_first, learning_first, extra_decay_first.T),
        (
            query_second,
            key_second,
            value_second,
            decay_second,
            learning_second,
            extra_decay_second.T,
        ),
    )
    entries = chunk_reads(solved, reads, begin_1, begin_2, value_first, value_second)
    prefix, (entry_1, inner_1, entry_2, inner_2) = sequence_prefix(total, entries)
    params = jnp.stack(
        [head_norm_gain_first, self_weight_first, head_norm_gain_second, self_weight_second]
    )
    mixer = mixer_outputs(
        prefix,
        (
            (entry_1, inner_1, sq1, sz1, query_first, key_first, value_first, output_gate_first),
            (entry_2, inner_2, sq2, sz2, query_second, key_second, value_second, output_gate_second),
        ),
        params,
    )
    rows = lax.all_to_all(mixer.reshape(-1, count, 2 * LANES), TP, 0, 0, tiled=True)
    middle = project(
        rows, output_projection_first, output_projection_second, stream, middle_norm_gain
    )

    nx = lax.axis_size("x")
    half = count // 2
    near_p = shift(middle, "x", 1, nx, True)
    near_m = shift(middle, "x", -1, nx, True)
    far = jnp.concatenate(
        [shift(near_p[:half], "x", 1, nx, True), shift(near_m[half:], "x", -1, nx, True)], 0
    )
    near = jnp.concatenate([near_p, near_m], 0)
    own_there = swap_core(middle)
    near_there = swap_core(near)
    far_there = swap_core(far)

    far_part, far_send = channel(far, far_there, weights)
    far_back = swap_core(far_send)
    near_part, near_send = channel(near, near_there, weights)
    near_back = swap_core(near_send)
    own_part, own_send = channel(middle, own_there, weights)
    own_back = swap_core(own_send)

    def total_of(part, back, at, more=None):
        out = part[at : at + half].astype(F32) + back[at : at + half].astype(F32)
        if more is not None:
            out = out + more.astype(F32)
        return out.astype(BF16)

    from_p = shift(total_of(far_part, far_back, 0), "x", 1, nx, True)
    from_m = shift(total_of(far_part, far_back, half), "x", -1, nx, True)
    back_p_first = shift(total_of(near_part, near_back, 0), "x", -1, nx, True)
    back_m_second = shift(total_of(near_part, near_back, 3 * half), "x", 1, nx, True)
    back_p_second = shift(total_of(near_part, near_back, half, from_m), "x", -1, nx, True)
    back_m_first = shift(total_of(near_part, near_back, 2 * half, from_p), "x", 1, nx, True)
    ff_total = (
        own_part.astype(F32)
        + own_back.astype(F32)
        + jnp.concatenate([back_p_first, back_p_second], 0).astype(F32)
        + jnp.concatenate([back_m_first, back_m_second], 0).astype(F32)
    )
    return norm_rows(ALPHA * middle.astype(F32) + ff_total, final_norm_gain).astype(BF16)


def solution(mesh):
    split = Mesh(mesh.devices.reshape(8, 4, 4, 2), ALL)
    long = P(SP, TP)
    group = (long,) * 7 + (P(TP), P(TP))
    return jax.shard_map(
        local,
        mesh=split,
        in_specs=(P(ALL, None),)
        + group
        + group
        + (P(), P(), P(), P(SP, TP), P(TP, SP), P()),
        out_specs=P(ALL, None),
        check_vma=False,
    )
```

```python
import jax
import jax.numpy as jnp
from jax import lax
from jax.experimental import pallas as pl
from jax.experimental.pallas import tpu as pltpu
from jax.sharding import Mesh
from jax.sharding import PartitionSpec as P


CHUNK = 64
LANES = 128
FIRST_HEAD_SIZE = 64
SECOND_HEAD_SIZE = 128
SP = ("z", "y")
TP = ("x", "c")
ALL = ("z", "y", "x", "c")
EPS_KEY = 1e-05
EPS_HEAD = 0.00064
EPS_NORM = 1e-05
ALPHA = 2.0**0.25
F32 = jnp.float32
BF16 = jnp.bfloat16


def mm(a, b):
    return jnp.dot(a.astype(BF16), b.astype(BF16), preferred_element_type=F32)


def mm_nt(a, b):
    return lax.dot_general(
        a.astype(BF16), b.astype(BF16), (((1,), (1,)), ((), ())), preferred_element_type=F32
    )


def mm_tn(a, b):
    return lax.dot_general(
        a.astype(BF16), b.astype(BF16), (((0,), (0,)), ((), ())), preferred_element_type=F32
    )


def iotas(rows=LANES, cols=LANES):
    return (
        lax.broadcasted_iota(jnp.int32, (rows, cols), 0),
        lax.broadcasted_iota(jnp.int32, (rows, cols), 1),
    )


def halves(rows):
    return lax.broadcasted_iota(jnp.int32, (rows, LANES), 1) < FIRST_HEAD_SIZE


def head_mean(array, pair):
    if not pair:
        return jnp.mean(array, -1, keepdims=True)
    low = halves(array.shape[0])
    first = jnp.sum(jnp.where(low, array, 0.0), -1, keepdims=True)
    second = jnp.sum(jnp.where(low, 0.0, array), -1, keepdims=True)
    return jnp.where(low, first, second) / FIRST_HEAD_SIZE


def spread(array):
    low = halves(array.shape[0])
    return jnp.concatenate([jnp.where(low, array, 0.0), jnp.where(low, 0.0, array)], 0)


def features(q_ref, k_ref, v_ref, d_ref, l_ref, e_ref, pair):
    q, k, v = (r[...].astype(F32) for r in (q_ref, k_ref, v_ref))
    size = FIRST_HEAD_SIZE if pair else SECOND_HEAD_SIZE
    normed = k * lax.rsqrt(head_mean(k * k, pair) + EPS_KEY) * size ** (-0.5)
    learn = jax.nn.sigmoid(l_ref[...].astype(F32))
    heads = e_ref.shape[0]
    rows, cols = iotas(heads, LANES)
    owner = (cols // size == rows).astype(BF16)
    burst = sum(mm_tn(part, owner) for part in split3(e_ref[...]))
    logdec = jax.nn.sigmoid(d_ref[...].astype(F32)) * (-(2.718281828459045**-0.5)) + burst
    return q, k, v, normed, learn, logdec


def split3(array):
    high = array.astype(BF16)
    rest = array - high.astype(F32)
    mid = rest.astype(BF16)
    return high, mid, (rest - mid.astype(F32)).astype(BF16)


def running_sum(logdec):
    rows, cols = iotas()
    tri = ((rows // CHUNK == cols // CHUNK) & (cols <= rows)).astype(BF16)
    return jnp.concatenate(
        [
            sum(mm(tri, part) for part in split3(logdec[at : at + LANES]))
            for at in range(0, logdec.shape[0], LANES)
        ],
        0,
    )


def chunk_row(array, at):
    return jnp.concatenate(
        [
            jnp.broadcast_to(array[c * CHUNK + at : c * CHUNK + at + 1], (CHUNK, array.shape[1]))
            for c in range(array.shape[0] // CHUNK)
        ],
        0,
    )


def inverses(lowers):
    rows, cols = iotas()
    eye = (rows == cols).astype(F32)
    found = [eye + jnp.where(rows // 2 == cols // 2, low, 0.0) for low in lowers]
    step = 2
    while step < CHUNK:
        mask = (rows // (2 * step) == cols // (2 * step)) & (rows // step != cols // step)
        short = [x.astype(BF16) for x in found]
        part = [mm(x, jnp.where(mask, low, 0.0)) for x, low in zip(short, lowers)]
        found = [f + mm(p, x) for f, p, x in zip(found, part, short)]
        step *= 2
    return found


def maps_kernel(*refs):
    ins, outs, carry = refs[:12], refs[12:21], refs[21]
    solved_ref, reads_ref, begin_1, begin_2, starts_q1, starts_z1, starts_q2, starts_z2, total = outs
    tokens = begin_1.shape[0]
    blocks, chunks = tokens // LANES, tokens // CHUNK
    step = pl.program_id(0)
    rows, cols = iotas()
    same = rows // CHUNK == cols // CHUNK
    strict = same & (cols < rows)
    inclusive = same & (cols <= rows)

    @pl.when(step == 0)
    def _():
        for g in range(2):
            carry[g, :LANES, :] = (rows == cols).astype(F32)
            carry[g, LANES:, :] = jnp.zeros((LANES, LANES), F32)

    units = [None] * (3 * blocks)
    keeps = []
    for g in range(2):
        q, k, v, normed, learn, logdec = features(*ins[6 * g : 6 * g + 6], g == 0)
        forward, backward = -normed, normed * learn
        cumul = running_sum(logdec)
        before = cumul - logdec
        middle = chunk_row(cumul, CHUNK // 2)
        ending = chunk_row(cumul, CHUNK - 1)
        up, down, left = jnp.exp(before - middle), jnp.exp(middle - cumul), jnp.exp(ending - cumul)
        keeps.append(
            [jnp.exp(cumul[(c + 1) * CHUNK - 1 : (c + 1) * CHUNK]) for c in range(chunks)]
        )
        (begin_1, begin_2)[g][...] = (q * jnp.exp(cumul)).astype(BF16)
        parts = (
            forward * up,
            q * jnp.exp(cumul - middle),
            backward * down,
            k * down,
            forward * jnp.exp(before),
            backward * left,
            k * left,
            v,
        )
        for b in range(blocks):
            if g == 0:
                for c in range(2):
                    at = b * LANES + c * CHUNK
                    units[3 * b + c] = [spread(p[at : at + CHUNK]).astype(BF16) for p in parts]
            else:
                units[3 * b + 2] = [p[b * LANES : (b + 1) * LANES].astype(BF16) for p in parts]
    grams = [
        mm_nt(jnp.concatenate([u[0], u[1]], 0), jnp.concatenate([u[2], u[3]], 0)) for u in units
    ]
    lowers = [jnp.where(strict, m[:LANES, :LANES], 0.0) for m in grams]
    writes = [jnp.where(strict, m[:LANES, LANES:], 0.0) for m in grams]
    for n, m in enumerate(grams):
        reads_ref[n, :, :LANES] = jnp.where(inclusive, m[LANES:, :LANES], 0.0).astype(BF16)
        reads_ref[n, :, LANES:] = jnp.where(inclusive, m[LANES:, LANES:], 0.0).astype(BF16)
    solvers = inverses(lowers)
    sides = [
        jnp.concatenate([u[4], mm(w, u[7]).astype(BF16)], 1) for u, w in zip(units, writes)
    ]
    solved = [mm(x, s).astype(BF16) for x, s in zip(solvers, sides)]
    moved = [[], []]
    for n, (u, s) in enumerate(zip(units, solved)):
        solved_ref[n] = s
        g = int(n % 3 == 2)
        for c in range(1 + g):
            at = slice(c * CHUNK, (c + 1) * CHUNK) if g else slice(0, LANES)
            both = mm_tn(s[at], u[5][at])
            moved[g].append((both[:LANES], both[LANES:] + mm_tn(u[7][at], u[6][at])))
    held = [carry[0], carry[1]]
    for c in range(chunks):
        for g, (sq, sz) in enumerate(((starts_q1, starts_z1), (starts_q2, starts_z2))):
            sq[c] = held[g][:LANES].astype(BF16)
            sz[c] = held[g][LANES:]
            transit, update = moved[g][c]
            after = held[g] * keeps[g][c] + mm(held[g], transit)
            held[g] = jnp.concatenate([after[:LANES], after[LANES:] + update], 0)
    for g in range(2):
        carry[g] = held[g]

    @pl.when(step == pl.num_programs(0) - 1)
    def _():
        total[...] = pack(held)


def chunk_maps(first, second):
    tokens = first[0].shape[0]
    block = 384
    chunks = tokens // CHUNK
    units = 3 * tokens // LANES
    rows = pl.BlockSpec((block, LANES), lambda i: (i, 0))
    state = pl.BlockSpec((block // CHUNK, LANES, LANES), lambda i: (i, 0, 0))
    unit = pl.BlockSpec((3 * block // LANES, LANES, 2 * LANES), lambda i: (i, 0, 0))
    ins = []
    for group in (first, second):
        ins += [rows] * 5 + [pl.BlockSpec((group[5].shape[0], block), lambda i: (0, i))]
    return pl.pallas_call(
        maps_kernel,
        grid=(tokens // block,),
        in_specs=ins,
        out_specs=[unit] * 2
        + [rows] * 2
        + [state] * 4
        + [pl.BlockSpec((384, LANES), lambda i: (0, 0))],
        out_shape=[jax.ShapeDtypeStruct((units, LANES, 2 * LANES), BF16)] * 2
        + [jax.ShapeDtypeStruct((tokens, LANES), BF16)] * 2
        + [jax.ShapeDtypeStruct((chunks, LANES, LANES), t) for t in (BF16, F32, BF16, F32)]
        + [jax.ShapeDtypeStruct((384, LANES), BF16)],
        scratch_shapes=[pltpu.VMEM((2, 2 * LANES, LANES), F32)],
        cost_estimate=pl.CostEstimate(
            flops=12_000_000_000, bytes_accessed=8_000_000, transcendentals=2_000_000
        ),
        name="chunk_maps",
    )(*first, *second)


def reads_kernel(
    solved, reads, begin_1, begin_2, v_1, v_2, sq1, sz1, sq2, sz2, entry_1, inner_1, entry_2, inner_2
):
    def store(at, entry, inner, sq, sz, entry_out, inner_out):
        for c in range(entry.shape[0] // CHUNK):
            part = slice(c * CHUNK, (c + 1) * CHUNK)
            rows = slice(at + c * CHUNK, at + (c + 1) * CHUNK)
            n = at // CHUNK + c
            short = entry[part].astype(BF16)
            entry_out[rows] = mm_nt(short, sq[n]).astype(BF16)
            inner_out[rows] = inner[part] + mm_nt(short, sz[n])

    for b in range(begin_1.shape[0] // LANES):
        for u in range(3):
            n = 3 * b + u
            at = slice(b * LANES + u * CHUNK, b * LANES + (u + 1) * CHUNK)
            if u == 2:
                at = slice(b * LANES, (b + 1) * LANES)
            value = v_2[at] if u == 2 else spread(v_1[at].astype(F32)).astype(BF16)
            carried = mm(reads[n, :, :LANES], solved[n])
            entry = carried[:, :LANES]
            inner = carried[:, LANES:] + mm(reads[n, :, LANES:], value)
            if u == 2:
                entry = begin_2[at].astype(F32) + entry
                store(at.start, entry, inner, sq2, sz2, entry_2, inner_2)
            else:
                entry = begin_1[at].astype(F32) + entry[:CHUNK] + entry[CHUNK:]
                inner = inner[:CHUNK] + inner[CHUNK:]
                store(at.start, entry, inner, sq1, sz1, entry_1, inner_1)


def chunk_reads(solved, reads, begin_1, begin_2, v_1, v_2, *starts):
    tokens = begin_1.shape[0]
    block = 256
    rows = pl.BlockSpec((block, LANES), lambda i: (i, 0))
    unit = pl.BlockSpec((3 * block // LANES, LANES, 2 * LANES), lambda i: (i, 0, 0))
    state = pl.BlockSpec((block // CHUNK, LANES, LANES), lambda i: (i, 0, 0))
    return pl.pallas_call(
        reads_kernel,
        grid=(tokens // block,),
        in_specs=[unit, unit] + [rows] * 4 + [state] * 4,
        out_specs=[rows] * 4,
        out_shape=[jax.ShapeDtypeStruct((tokens, LANES), t) for t in (BF16, F32, BF16, F32)],
        cost_estimate=pl.CostEstimate(
            flops=4_000_000_000, bytes_accessed=6_000_000, transcendentals=0
        ),
        name="chunk_reads",
    )(solved, reads, begin_1, begin_2, v_1, v_2, *starts)


def unpack(packed):
    def widen(part):
        return spread(part.astype(F32))

    return (
        jnp.concatenate([widen(packed[0:64]), widen(packed[64:128])], 0),
        packed[128:384].astype(F32),
    )


def pack(pairs):
    first, second = pairs
    return jnp.concatenate(
        [first[0:64] + first[64:128], first[128:192] + first[192:256], second], 0
    ).astype(BF16)


def compose(earlier, later):
    out = []
    for a, b in zip(earlier, later):
        moved = mm(a, b[:LANES])
        out.append(jnp.concatenate([moved[:LANES], moved[LANES:] + b[LANES:]], 0))
    return out


def row_kernel(mine_ref, own, one, two, three, before_ref, total_ref):
    mine = mine_ref[0]
    by_shift = [r[...] for r in (own, one, two, three)]

    def member(k):
        shift = lax.rem(mine - k + 4, 4)
        out = by_shift[3]
        for s in range(3):
            out = jnp.where(shift == s, by_shift[s], out)
        return unpack(out)

    rows, cols = iotas()
    eye = (rows == cols).astype(F32)
    neutral = jnp.concatenate([eye, jnp.zeros((LANES, LANES), F32)], 0)
    running = member(0)
    before = [jnp.where(mine == 0, neutral, r) for r in running]
    for k in range(1, 4):
        before = [jnp.where(mine == k, r, b) for r, b in zip(running, before)] if k > 1 else [
            jnp.where(mine == 0, neutral, r) for r in running
        ]
        running = compose(running, member(k))
    before_ref[...] = pack(before)
    total_ref[...] = pack(running)


def vmem_call(kernel, out_shape, *args, scalars=0):
    return pl.pallas_call(
        kernel,
        in_specs=[pl.BlockSpec(memory_space=pltpu.SMEM)] * scalars
        + [pl.BlockSpec(memory_space=pltpu.VMEM)] * (len(args) - scalars),
        out_specs=jax.tree.map(lambda _: pl.BlockSpec(memory_space=pltpu.VMEM), out_shape),
        out_shape=out_shape,
    )(*args)


def join_kernel(earlier_ref, later_ref, out_ref):
    out_ref[...] = pack(compose(unpack(earlier_ref[...]), unpack(later_ref[...])))


def join_two_kernel(earlier_ref, before_ref, through_ref, before_out, through_out):
    earlier = unpack(earlier_ref[...])
    before_out[...] = pack(compose(earlier, unpack(before_ref[...])))
    through = pack(compose(earlier, unpack(through_ref[...])))
    through_out[0:64] = through[64:128]
    through_out[64:192] = through[256:384]


def shift(array, axis, by, size, wrap):
    pairs = [(i, (i + by) % size) for i in range(size) if wrap or 0 <= i + by < size]
    return lax.ppermute(array, axis, pairs)


def sequence_prefix(total, entries):
    shape = jax.ShapeDtypeStruct(total.shape, BF16)
    ny, nz = lax.axis_size("y"), lax.axis_size("z")
    peers = [shift(total, "y", s, ny, True) for s in (1, 2, 3)]
    peers, entries = lax.optimization_barrier((peers, entries))
    mine = lax.axis_index("y").astype(jnp.int32).reshape(1)
    row_before, row_total = vmem_call(row_kernel, (shape, shape), mine, total, *peers, scalars=1)
    before = shift(row_total, "z", 1, nz, False)
    through = vmem_call(join_kernel, shape, before, row_total)
    earlier = shift(through, "z", 2, nz, False)
    short = jax.ShapeDtypeStruct((192, LANES), BF16)
    before, send = vmem_call(join_two_kernel, (shape, short), earlier, before, through)
    last = shift(send, "z", 4, nz, False)
    return (last, before, row_before), entries


def outputs_kernel(*refs):
    (last, before, row_before), ins, out, states = refs[:3], refs[3:15], refs[15], refs[16]

    @pl.when(pl.program_id(0) == 0)
    def _():
        near = unpack(before[...])
        row = unpack(row_before[...])
        far = (spread(last[0:64].astype(F32)), last[64:192])
        for g in range(2):
            start = mm(far[g], near[g][:LANES]) + near[g][LANES:]
            states[g] = mm(start, row[g][:LANES]) + row[g][LANES:]

    for g in range(2):
        entry, inner, q_ref, k_ref, v_ref, gate_ref = ins[6 * g : 6 * g + 6]
        pair = g == 0
        gain, weight = out_params(refs, g)
        heady = mm_nt(entry[...], states[g]) + inner[...]
        q, k, v, gate = (r[...].astype(F32) for r in (q_ref, k_ref, v_ref, gate_ref))
        centred = heady - head_mean(heady, pair)
        spread_ = head_mean(centred * centred, pair)
        normalized = centred * lax.rsqrt(spread_ + EPS_HEAD) * gain
        size = FIRST_HEAD_SIZE if pair else SECOND_HEAD_SIZE
        extra = head_mean(q * k * weight, pair) * size * v
        out[:, g * LANES : (g + 1) * LANES] = (
            (normalized + extra) * jax.nn.sigmoid(gate)
        ).astype(BF16)


def out_params(refs, g):
    params = refs[17]
    return params[2 * g : 2 * g + 1], params[2 * g + 1 : 2 * g + 2]


def mixer_outputs(prefix, groups, params):
    tokens = groups[0][0].shape[0]
    block = 256
    rows = pl.BlockSpec((block, LANES), lambda i: (i, 0))

    def whole(a):
        return pl.BlockSpec(a.shape, lambda i: (0,) * a.ndim)

    def kernel(*refs):
        ins, out, states = refs[:16], refs[16], refs[17]
        outputs_kernel(*ins[:15], out, states, ins[15])

    return pl.pallas_call(
        kernel,
        grid=(tokens // block,),
        in_specs=[whole(a) for a in prefix]
        + [rows] * 12
        + [whole(params)],
        out_specs=pl.BlockSpec((block, 2 * LANES), lambda i: (i, 0)),
        out_shape=jax.ShapeDtypeStruct((tokens, 2 * LANES), BF16),
        scratch_shapes=[pltpu.VMEM((2, LANES, LANES), F32)],
        cost_estimate=pl.CostEstimate(
            flops=2_000_000_000, bytes_accessed=6_000_000, transcendentals=300_000
        ),
        name="mixer_outputs",
    )(*prefix, *groups[0], *groups[1], params)


def norm_rows(array, gain):
    mean_part = jnp.mean(array, -1, keepdims=True)
    centred = array - mean_part
    return centred * lax.rsqrt(jnp.mean(centred * centred, -1, keepdims=True) + EPS_NORM) * gain


def project_kernel(rows_ref, stream_ref, gain_ref, first, second, out_ref, held, sems):
    peers = rows_ref.shape[0]
    copies = []
    for n in range(peers):
        at = pl.ds(n * LANES, LANES)
        for side, source in enumerate((first, second)):
            copies.append(
                pltpu.make_async_copy(
                    source.at[at, :],
                    held.at[n, pl.ds(side * LANES, LANES), :],
                    sems.at[n, side],
                )
            )
    for copy in copies:
        copy.start()
    total = ALPHA * stream_ref[...].astype(F32)
    for n in range(peers):
        copies[2 * n].wait()
        copies[2 * n + 1].wait()
        total += jnp.dot(rows_ref[n], held[n], preferred_element_type=F32)
    out_ref[...] = norm_rows(total, gain_ref[...]).astype(BF16)


def project(rows, first, second, stream, gain):
    peers, count, _ = rows.shape
    width = first.shape[1]
    near = pl.BlockSpec(memory_space=pltpu.VMEM)
    far = pl.BlockSpec(memory_space=pl.ANY)
    return pl.pallas_call(
        project_kernel,
        in_specs=[near, near, near, far, far],
        out_specs=near,
        out_shape=jax.ShapeDtypeStruct((count, width), BF16),
        scratch_shapes=[
            pltpu.VMEM((peers, 2 * LANES, width), BF16),
            pltpu.SemaphoreType.DMA((peers, 2)),
        ],
        cost_estimate=pl.CostEstimate(
            flops=4_000_000_000, bytes_accessed=9_000_000, transcendentals=100
        ),
        name="project",
    )(rows, stream, gain.reshape(1, -1), first, second)


def swap_core(array):
    return lax.ppermute(array, "c", [(0, 1), (1, 0)])


def channel_kernel(*refs):
    blocks, refs = refs[:-9], refs[-9:]
    weights, outs, (rows, acc, held, sems) = refs[0], refs[1:5], refs[5:]
    pieces, group, depth, _ = held.shape
    half = pieces // 2
    block = group * depth
    copies = []
    for n in range(pieces):
        side = weights.at[
            pl.ds((n % half) * group, group), pl.ds((n // half) * depth, depth), :
        ]
        copies.append(pltpu.make_async_copy(side, held.at[n], sems.at[n]))
    for copy in copies:
        copy.start()
    start = 0
    for ref in blocks:
        for n in range(half):
            rows[n, start : start + ref.shape[0]] = ref[:, n * block : (n + 1) * block]
        start += ref.shape[0]
    for n in range(half):
        copies[n].wait()
        part = jnp.dot(rows[n], held[n].reshape(block, -1), preferred_element_type=F32)
        acc[...] = part if n == 0 else acc[...] + part
    hidden = jnp.square(jnp.maximum(acc[...], 0.0)).astype(BF16)
    for n in range(half):
        copies[half + n].wait()
        part = mm_nt(hidden, held[half + n].reshape(block, -1)).astype(BF16)
        start = 0
        for out in outs:
            out[:, n * block : (n + 1) * block] = part[start : start + out.shape[0]]
            start += out.shape[0]


def channel(blocks, weights):
    peers, depth, hidden = weights.shape
    width = blocks[0].shape[1]
    count = sum(b.shape[0] for b in blocks) // 2
    pieces = 8
    near = pl.BlockSpec(memory_space=pltpu.VMEM)
    return pl.pallas_call(
        channel_kernel,
        in_specs=[near] * len(blocks) + [pl.BlockSpec(memory_space=pl.ANY)],
        out_specs=[near] * 4,
        out_shape=[
            jax.ShapeDtypeStruct((rows, width), BF16) for rows in (3 * count // 4, count // 4) * 2
        ],
        scratch_shapes=[
            pltpu.VMEM((pieces // 2, 2 * count, 2 * width // pieces), BF16),
            pltpu.VMEM((2 * count, hidden), F32),
            pltpu.VMEM((pieces, 2 * peers // pieces, depth // 2, hidden), BF16),
            pltpu.SemaphoreType.DMA((pieces,)),
        ],
        cost_estimate=pl.CostEstimate(
            flops=8 * count * width * hidden,
            bytes_accessed=2 * peers * depth * hidden,
            transcendentals=0,
        ),
        name="channel",
    )(*blocks, weights)


def layer(
    stream,
    query_first,
    key_first,
    value_first,
    decay_first,
    learning_first,
    output_gate_first,
    extra_decay_first,
    head_norm_gain_first,
    self_weight_first,
    query_second,
    key_second,
    value_second,
    decay_second,
    learning_second,
    output_gate_second,
    extra_decay_second,
    head_norm_gain_second,
    self_weight_second,
    output_projection_first,
    output_projection_second,
    middle_norm_gain,
    mixer_up_weight,
    mixer_down_weight,
    final_norm_gain,
):
    count, _ = stream.shape
    both = jnp.concatenate([mixer_up_weight, mixer_down_weight.T], 0)
    weights = lax.all_gather(both, SP)

    solved, reads, begin_1, begin_2, sq1, sz1, sq2, sz2, total = chunk_maps(
        (query_first, key_first, value_first, decay_first, learning_first, extra_decay_first.T),
        (
            query_second,
            key_second,
            value_second,
            decay_second,
            learning_second,
            extra_decay_second.T,
        ),
    )
    entries = chunk_reads(
        solved, reads, begin_1, begin_2, value_first, value_second, sq1, sz1, sq2, sz2
    )
    prefix, (entry_1, inner_1, entry_2, inner_2) = sequence_prefix(total, entries)
    params = jnp.stack(
        [head_norm_gain_first, self_weight_first, head_norm_gain_second, self_weight_second]
    )
    mixer = mixer_outputs(
        prefix,
        (
            (entry_1, inner_1, query_first, key_first, value_first, output_gate_first),
            (entry_2, inner_2, query_second, key_second, value_second, output_gate_second),
        ),
        params,
    )
    rows = lax.all_to_all(mixer.reshape(-1, count, 2 * LANES), TP, 0, 0, tiled=True)
    middle = project(
        rows, output_projection_first, output_projection_second, stream, middle_norm_gain
    )

    nx = lax.axis_size("x")
    half = count // 2
    own_there = swap_core(middle)
    near_p = shift(middle, "x", 1, nx, True)
    near_m = shift(middle, "x", -1, nx, True)
    far = jnp.concatenate(
        [shift(near_p[:half], "x", 1, nx, True), shift(near_m[half:], "x", -1, nx, True)], 0
    )
    near = jnp.concatenate([near_p, near_m], 0)
    near_there = swap_core(near)
    far_there = swap_core(far)
    near_part, far_part, near_send, far_send = channel(
        (middle, near, far, own_there, near_there, far_there), weights
    )
    far_back = swap_core(far_send)
    near_back = swap_core(near_send)

    def total_of(part, back, n):
        at = slice(n * count, (n + 1) * count)
        return part[at].astype(F32) + back[at].astype(F32)

    from_far = shift(total_of(far_part, far_back, 0).astype(BF16), "x", 2, nx, True)
    from_p = shift(total_of(near_part, near_back, 1).astype(BF16), "x", -1, nx, True)
    from_m = shift(total_of(near_part, near_back, 2).astype(BF16), "x", 1, nx, True)
    ff_total = total_of(near_part, near_back, 0)
    for part in (from_far, from_p, from_m):
        ff_total = ff_total + part.astype(F32)
    return norm_rows(ALPHA * middle.astype(F32) + ff_total, final_norm_gain).astype(BF16)


def solution(mesh):
    split = Mesh(mesh.devices.reshape(8, 4, 4, 2), ALL)
    long = P(SP, TP)
    group = (long,) * 7 + (P(TP), P(TP))
    return jax.shard_map(
        layer,
        mesh=split,
        in_specs=(P(ALL, None),)
        + group
        + group
        + (P(), P(), P(), P(SP, TP), P(TP, SP), P()),
        out_specs=P(ALL, None),
        check_vma=False,
    )
```

```python
import jax
import jax.numpy as jnp
from jax import lax
from jax.experimental import pallas as pl
from jax.experimental.pallas import tpu as pltpu
from jax.sharding import Mesh
from jax.sharding import PartitionSpec as P


CHUNK = 64
LANES = 128
FIRST_HEAD_SIZE = 64
SECOND_HEAD_SIZE = 128
SP = ("z", "y")
TP = ("x", "c")
ALL = ("z", "y", "x", "c")
EPS_KEY = 1e-05
EPS_HEAD = 0.00064
EPS_NORM = 1e-05
ALPHA = 2.0**0.25
F32 = jnp.float32
BF16 = jnp.bfloat16


def mm(a, b):
    return jnp.dot(a.astype(BF16), b.astype(BF16), preferred_element_type=F32)


def mm_nt(a, b):
    return lax.dot_general(
        a.astype(BF16), b.astype(BF16), (((1,), (1,)), ((), ())), preferred_element_type=F32
    )


def mm_tn(a, b):
    return lax.dot_general(
        a.astype(BF16), b.astype(BF16), (((0,), (0,)), ((), ())), preferred_element_type=F32
    )


def iotas(rows=LANES, cols=LANES):
    return (
        lax.broadcasted_iota(jnp.int32, (rows, cols), 0),
        lax.broadcasted_iota(jnp.int32, (rows, cols), 1),
    )


def halves(rows):
    return lax.broadcasted_iota(jnp.int32, (rows, LANES), 1) < FIRST_HEAD_SIZE


def head_mean(array, pair):
    if not pair:
        return jnp.mean(array, -1, keepdims=True)
    low = halves(array.shape[0])
    first = jnp.sum(jnp.where(low, array, 0.0), -1, keepdims=True)
    second = jnp.sum(jnp.where(low, 0.0, array), -1, keepdims=True)
    return jnp.where(low, first, second) / FIRST_HEAD_SIZE


def spread(array):
    low = halves(array.shape[0])
    return jnp.concatenate([jnp.where(low, array, 0.0), jnp.where(low, 0.0, array)], 0)


def features(q_ref, k_ref, v_ref, d_ref, l_ref, e_ref, pair):
    q, k, v = (r[...].astype(F32) for r in (q_ref, k_ref, v_ref))
    size = FIRST_HEAD_SIZE if pair else SECOND_HEAD_SIZE
    normed = k * lax.rsqrt(head_mean(k * k, pair) + EPS_KEY) * size ** (-0.5)
    learn = jax.nn.sigmoid(l_ref[...].astype(F32))
    heads = e_ref.shape[0]
    rows, cols = iotas(heads, LANES)
    owner = (cols // size == rows).astype(BF16)
    burst = sum(mm_tn(part, owner) for part in split3(e_ref[...]))
    logdec = jax.nn.sigmoid(d_ref[...].astype(F32)) * (-(2.718281828459045**-0.5)) + burst
    return q, k, v, normed, learn, logdec


def split3(array):
    high = array.astype(BF16)
    rest = array - high.astype(F32)
    mid = rest.astype(BF16)
    return high, mid, (rest - mid.astype(F32)).astype(BF16)


def running_sum(logdec):
    rows, cols = iotas()
    tri = ((rows // CHUNK == cols // CHUNK) & (cols <= rows)).astype(BF16)
    return jnp.concatenate(
        [
            sum(mm(tri, part) for part in split3(logdec[at : at + LANES]))
            for at in range(0, logdec.shape[0], LANES)
        ],
        0,
    )


def chunk_row(array, at):
    return jnp.concatenate(
        [
            jnp.broadcast_to(array[c * CHUNK + at : c * CHUNK + at + 1], (CHUNK, array.shape[1]))
            for c in range(array.shape[0] // CHUNK)
        ],
        0,
    )


def inverses(lowers):
    rows, cols = iotas()
    eye = (rows == cols).astype(F32)
    found = [eye + jnp.where(rows // 2 == cols // 2, low, 0.0) for low in lowers]
    step = 2
    while step < CHUNK:
        mask = (rows // (2 * step) == cols // (2 * step)) & (rows // step != cols // step)
        short = [x.astype(BF16) for x in found]
        part = [mm(x, jnp.where(mask, low, 0.0)) for x, low in zip(short, lowers)]
        found = [f + mm(p, x) for f, p, x in zip(found, part, short)]
        step *= 2
    return found


def maps_kernel(*refs):
    ins, outs, carry = refs[:12], refs[12:21], refs[21]
    solved_ref, reads_ref, begin_1, begin_2, starts_q1, starts_z1, starts_q2, starts_z2, total = outs
    tokens = begin_1.shape[0]
    blocks, chunks = tokens // LANES, tokens // CHUNK
    step = pl.program_id(0)
    rows, cols = iotas()
    same = rows // CHUNK == cols // CHUNK
    strict = same & (cols < rows)
    inclusive = same & (cols <= rows)

    @pl.when(step == 0)
    def _():
        for g in range(2):
            carry[g, :LANES, :] = (rows == cols).astype(F32)
            carry[g, LANES:, :] = jnp.zeros((LANES, LANES), F32)

    units = [None] * (3 * blocks)
    keeps = []
    for g in range(2):
        q, k, v, normed, learn, logdec = features(*ins[6 * g : 6 * g + 6], g == 0)
        forward, backward = -normed, normed * learn
        cumul = running_sum(logdec)
        before = cumul - logdec
        middle = chunk_row(cumul, CHUNK // 2)
        ending = chunk_row(cumul, CHUNK - 1)
        up, down, left = jnp.exp(before - middle), jnp.exp(middle - cumul), jnp.exp(ending - cumul)
        keeps.append(
            [jnp.exp(cumul[(c + 1) * CHUNK - 1 : (c + 1) * CHUNK]) for c in range(chunks)]
        )
        (begin_1, begin_2)[g][...] = (q * jnp.exp(cumul)).astype(BF16)
        parts = (
            forward * up,
            q * jnp.exp(cumul - middle),
            backward * down,
            k * down,
            forward * jnp.exp(before),
            backward * left,
            k * left,
            v,
        )
        for b in range(blocks):
            if g == 0:
                for c in range(2):
                    at = b * LANES + c * CHUNK
                    units[3 * b + c] = [spread(p[at : at + CHUNK]).astype(BF16) for p in parts]
            else:
                units[3 * b + 2] = [p[b * LANES : (b + 1) * LANES].astype(BF16) for p in parts]
    grams = [
        mm_nt(jnp.concatenate([u[0], u[1]], 0), jnp.concatenate([u[2], u[3]], 0)) for u in units
    ]
    lowers = [jnp.where(strict, m[:LANES, :LANES], 0.0) for m in grams]
    writes = [jnp.where(strict, m[:LANES, LANES:], 0.0) for m in grams]
    for n, m in enumerate(grams):
        reads_ref[n, :, :LANES] = jnp.where(inclusive, m[LANES:, :LANES], 0.0).astype(BF16)
        reads_ref[n, :, LANES:] = jnp.where(inclusive, m[LANES:, LANES:], 0.0).astype(BF16)
    solvers = inverses(lowers)
    sides = [
        jnp.concatenate([u[4], mm(w, u[7]).astype(BF16)], 1) for u, w in zip(units, writes)
    ]
    solved = [mm(x, s).astype(BF16) for x, s in zip(solvers, sides)]
    moved = [[], []]
    for n, (u, s) in enumerate(zip(units, solved)):
        solved_ref[n] = s
        g = int(n % 3 == 2)
        for c in range(1 + g):
            at = slice(c * CHUNK, (c + 1) * CHUNK) if g else slice(0, LANES)
            both = mm_tn(s[at], u[5][at])
            moved[g].append((both[:LANES], both[LANES:] + mm_tn(u[7][at], u[6][at])))
    held = [carry[0], carry[1]]
    for c in range(chunks):
        for g, (sq, sz) in enumerate(((starts_q1, starts_z1), (starts_q2, starts_z2))):
            sq[c] = held[g][:LANES].astype(BF16)
            sz[c] = held[g][LANES:]
            transit, update = moved[g][c]
            after = held[g] * keeps[g][c] + mm(held[g], transit)
            held[g] = jnp.concatenate([after[:LANES], after[LANES:] + update], 0)
    for g in range(2):
        carry[g] = held[g]

    @pl.when(step == pl.num_programs(0) - 1)
    def _():
        total[...] = pack(held)


def chunk_maps(first, second):
    tokens = first[0].shape[0]
    block = 384
    chunks = tokens // CHUNK
    units = 3 * tokens // LANES
    rows = pl.BlockSpec((block, LANES), lambda i: (i, 0))
    state = pl.BlockSpec((block // CHUNK, LANES, LANES), lambda i: (i, 0, 0))
    unit = pl.BlockSpec((3 * block // LANES, LANES, 2 * LANES), lambda i: (i, 0, 0))
    ins = []
    for group in (first, second):
        ins += [rows] * 5 + [pl.BlockSpec((group[5].shape[0], block), lambda i: (0, i))]
    return pl.pallas_call(
        maps_kernel,
        grid=(tokens // block,),
        in_specs=ins,
        out_specs=[unit] * 2
        + [rows] * 2
        + [state] * 4
        + [pl.BlockSpec((384, LANES), lambda i: (0, 0))],
        out_shape=[jax.ShapeDtypeStruct((units, LANES, 2 * LANES), BF16)] * 2
        + [jax.ShapeDtypeStruct((tokens, LANES), BF16)] * 2
        + [jax.ShapeDtypeStruct((chunks, LANES, LANES), t) for t in (BF16, F32, BF16, F32)]
        + [jax.ShapeDtypeStruct((384, LANES), BF16)],
        scratch_shapes=[pltpu.VMEM((2, 2 * LANES, LANES), F32)],
        cost_estimate=pl.CostEstimate(
            flops=12_000_000_000, bytes_accessed=8_000_000, transcendentals=2_000_000
        ),
        name="chunk_maps",
    )(*first, *second)


def reads_kernel(
    solved, reads, begin_1, begin_2, v_1, v_2, sq1, sz1, sq2, sz2, entry_1, inner_1, entry_2, inner_2
):
    def store(at, entry, inner, sq, sz, entry_out, inner_out):
        for c in range(entry.shape[0] // CHUNK):
            part = slice(c * CHUNK, (c + 1) * CHUNK)
            rows = slice(at + c * CHUNK, at + (c + 1) * CHUNK)
            n = at // CHUNK + c
            short = entry[part].astype(BF16)
            entry_out[rows] = mm_nt(short, sq[n]).astype(BF16)
            inner_out[rows] = inner[part] + mm_nt(short, sz[n])

    for b in range(begin_1.shape[0] // LANES):
        for u in range(3):
            n = 3 * b + u
            at = slice(b * LANES + u * CHUNK, b * LANES + (u + 1) * CHUNK)
            if u == 2:
                at = slice(b * LANES, (b + 1) * LANES)
            value = v_2[at] if u == 2 else spread(v_1[at].astype(F32)).astype(BF16)
            carried = mm(reads[n, :, :LANES], solved[n])
            entry = carried[:, :LANES]
            inner = carried[:, LANES:] + mm(reads[n, :, LANES:], value)
            if u == 2:
                entry = begin_2[at].astype(F32) + entry
                store(at.start, entry, inner, sq2, sz2, entry_2, inner_2)
            else:
                entry = begin_1[at].astype(F32) + entry[:CHUNK] + entry[CHUNK:]
                inner = inner[:CHUNK] + inner[CHUNK:]
                store(at.start, entry, inner, sq1, sz1, entry_1, inner_1)


def chunk_reads(solved, reads, begin_1, begin_2, v_1, v_2, *starts):
    tokens = begin_1.shape[0]
    block = 384
    rows = pl.BlockSpec((block, LANES), lambda i: (i, 0))
    unit = pl.BlockSpec((3 * block // LANES, LANES, 2 * LANES), lambda i: (i, 0, 0))
    state = pl.BlockSpec((block // CHUNK, LANES, LANES), lambda i: (i, 0, 0))
    return pl.pallas_call(
        reads_kernel,
        grid=(tokens // block,),
        in_specs=[unit, unit] + [rows] * 4 + [state] * 4,
        out_specs=[rows] * 4,
        out_shape=[jax.ShapeDtypeStruct((tokens, LANES), t) for t in (BF16, F32, BF16, F32)],
        cost_estimate=pl.CostEstimate(
            flops=4_000_000_000, bytes_accessed=6_000_000, transcendentals=0
        ),
        name="chunk_reads",
    )(solved, reads, begin_1, begin_2, v_1, v_2, *starts)


def unpack(packed):
    def widen(part):
        return spread(part.astype(F32))

    return (
        jnp.concatenate([widen(packed[0:64]), widen(packed[64:128])], 0),
        packed[128:384].astype(F32),
    )


def pack(pairs):
    first, second = pairs
    return jnp.concatenate(
        [first[0:64] + first[64:128], first[128:192] + first[192:256], second], 0
    ).astype(BF16)


def compose(earlier, later):
    out = []
    for a, b in zip(earlier, later):
        moved = mm(a, b[:LANES])
        out.append(jnp.concatenate([moved[:LANES], moved[LANES:] + b[LANES:]], 0))
    return out


def row_kernel(mine_ref, own, one, two, three, before_ref, total_ref):
    mine = mine_ref[0]
    by_shift = [r[...] for r in (own, one, two, three)]

    def member(k):
        shift = lax.rem(mine - k + 4, 4)
        out = by_shift[3]
        for s in range(3):
            out = jnp.where(shift == s, by_shift[s], out)
        return unpack(out)

    rows, cols = iotas()
    eye = (rows == cols).astype(F32)
    neutral = jnp.concatenate([eye, jnp.zeros((LANES, LANES), F32)], 0)
    running = member(0)
    before = [jnp.where(mine == 0, neutral, r) for r in running]
    for k in range(1, 4):
        before = [jnp.where(mine == k, r, b) for r, b in zip(running, before)] if k > 1 else [
            jnp.where(mine == 0, neutral, r) for r in running
        ]
        running = compose(running, member(k))
    before_ref[...] = pack(before)
    total_ref[...] = pack(running)


def vmem_call(kernel, out_shape, *args, scalars=0):
    return pl.pallas_call(
        kernel,
        in_specs=[pl.BlockSpec(memory_space=pltpu.SMEM)] * scalars
        + [pl.BlockSpec(memory_space=pltpu.VMEM)] * (len(args) - scalars),
        out_specs=jax.tree.map(lambda _: pl.BlockSpec(memory_space=pltpu.VMEM), out_shape),
        out_shape=out_shape,
    )(*args)


def join_kernel(earlier_ref, later_ref, out_ref):
    out_ref[...] = pack(compose(unpack(earlier_ref[...]), unpack(later_ref[...])))


def join_two_kernel(earlier_ref, before_ref, through_ref, before_out, through_out):
    earlier = unpack(earlier_ref[...])
    before_out[...] = pack(compose(earlier, unpack(before_ref[...])))
    through = pack(compose(earlier, unpack(through_ref[...])))
    through_out[0:64] = through[64:128]
    through_out[64:192] = through[256:384]


def shift(array, axis, by, size, wrap):
    pairs = [(i, (i + by) % size) for i in range(size) if wrap or 0 <= i + by < size]
    return lax.ppermute(array, axis, pairs)


def sequence_prefix(total, entries):
    shape = jax.ShapeDtypeStruct(total.shape, BF16)
    ny, nz = lax.axis_size("y"), lax.axis_size("z")
    peers = [shift(total, "y", s, ny, True) for s in (1, 2, 3)]
    peers, entries = lax.optimization_barrier((peers, entries))
    mine = lax.axis_index("y").astype(jnp.int32).reshape(1)
    row_before, row_total = vmem_call(row_kernel, (shape, shape), mine, total, *peers, scalars=1)
    before = shift(row_total, "z", 1, nz, False)
    through = vmem_call(join_kernel, shape, before, row_total)
    earlier = shift(through, "z", 2, nz, False)
    short = jax.ShapeDtypeStruct((192, LANES), BF16)
    before, send = vmem_call(join_two_kernel, (shape, short), earlier, before, through)
    last = shift(send, "z", 4, nz, False)
    return (last, before, row_before), entries


def outputs_kernel(*refs):
    (last, before, row_before), ins, out, states = refs[:3], refs[3:15], refs[15], refs[16]

    @pl.when(pl.program_id(0) == 0)
    def _():
        near = unpack(before[...])
        row = unpack(row_before[...])
        far = (spread(last[0:64].astype(F32)), last[64:192])
        for g in range(2):
            start = mm(far[g], near[g][:LANES]) + near[g][LANES:]
            states[g] = mm(start, row[g][:LANES]) + row[g][LANES:]

    for g in range(2):
        entry, inner, q_ref, k_ref, v_ref, gate_ref = ins[6 * g : 6 * g + 6]
        pair = g == 0
        gain, weight = out_params(refs, g)
        heady = mm_nt(entry[...], states[g]) + inner[...]
        q, k, v, gate = (r[...].astype(F32) for r in (q_ref, k_ref, v_ref, gate_ref))
        centred = heady - head_mean(heady, pair)
        spread_ = head_mean(centred * centred, pair)
        normalized = centred * lax.rsqrt(spread_ + EPS_HEAD) * gain
        size = FIRST_HEAD_SIZE if pair else SECOND_HEAD_SIZE
        extra = head_mean(q * k * weight, pair) * size * v
        out[:, g * LANES : (g + 1) * LANES] = (
            (normalized + extra) * jax.nn.sigmoid(gate)
        ).astype(BF16)


def out_params(refs, g):
    params = refs[17]
    return params[2 * g : 2 * g + 1], params[2 * g + 1 : 2 * g + 2]


def mixer_outputs(prefix, groups, params):
    tokens = groups[0][0].shape[0]
    block = 384
    rows = pl.BlockSpec((block, LANES), lambda i: (i, 0))

    def whole(a):
        return pl.BlockSpec(a.shape, lambda i: (0,) * a.ndim)

    def kernel(*refs):
        ins, out, states = refs[:16], refs[16], refs[17]
        outputs_kernel(*ins[:15], out, states, ins[15])

    return pl.pallas_call(
        kernel,
        grid=(tokens // block,),
        in_specs=[whole(a) for a in prefix]
        + [rows] * 12
        + [whole(params)],
        out_specs=pl.BlockSpec((block, 2 * LANES), lambda i: (i, 0)),
        out_shape=jax.ShapeDtypeStruct((tokens, 2 * LANES), BF16),
        scratch_shapes=[pltpu.VMEM((2, LANES, LANES), F32)],
        cost_estimate=pl.CostEstimate(
            flops=2_000_000_000, bytes_accessed=6_000_000, transcendentals=300_000
        ),
        name="mixer_outputs",
    )(*prefix, *groups[0], *groups[1], params)


def norm_rows(array, gain):
    mean_part = jnp.mean(array, -1, keepdims=True)
    centred = array - mean_part
    return centred * lax.rsqrt(jnp.mean(centred * centred, -1, keepdims=True) + EPS_NORM) * gain


def project_kernel(rows_ref, stream_ref, gain_ref, first, second, out_ref, held, sems):
    peers = rows_ref.shape[0]
    copies = []
    for n in range(peers):
        at = pl.ds(n * LANES, LANES)
        for side, source in enumerate((first, second)):
            copies.append(
                pltpu.make_async_copy(
                    source.at[at, :],
                    held.at[n, pl.ds(side * LANES, LANES), :],
                    sems.at[n, side],
                )
            )
    for copy in copies:
        copy.start()
    total = ALPHA * stream_ref[...].astype(F32)
    for n in range(peers):
        copies[2 * n].wait()
        copies[2 * n + 1].wait()
        total += jnp.dot(rows_ref[n], held[n], preferred_element_type=F32)
    out_ref[...] = norm_rows(total, gain_ref[...]).astype(BF16)


def project(rows, first, second, stream, gain):
    peers, count, _ = rows.shape
    width = first.shape[1]
    near = pl.BlockSpec(memory_space=pltpu.VMEM)
    far = pl.BlockSpec(memory_space=pl.ANY)
    return pl.pallas_call(
        project_kernel,
        in_specs=[near, near, near, far, far],
        out_specs=near,
        out_shape=jax.ShapeDtypeStruct((count, width), BF16),
        scratch_shapes=[
            pltpu.VMEM((peers, 2 * LANES, width), BF16),
            pltpu.SemaphoreType.DMA((peers, 2)),
        ],
        cost_estimate=pl.CostEstimate(
            flops=4_000_000_000, bytes_accessed=9_000_000, transcendentals=100
        ),
        name="project",
    )(rows, stream, gain.reshape(1, -1), first, second)


def swap_core(array):
    return lax.ppermute(array, "c", [(0, 1), (1, 0)])


def channel_kernel(*refs):
    blocks, weights, outs = refs[:6], refs[6], refs[7:11]
    rows, acc, held, ready, row_sems, sems, out_sems = refs[11:]
    pieces, group, depth, _ = held.shape
    half = pieces // 2
    block = group * depth

    def columns(ref, n):
        return ref.at[:, pl.ds(n * block, block)]

    def spans(refs):
        start = 0
        for m, ref in enumerate(refs):
            yield m, ref, pl.ds(start, ref.shape[0])
            start += ref.shape[0]

    copies, row_copies, out_copies = [], [], []
    for n in range(pieces):
        if n < half:
            row_copies.append(
                [
                    pltpu.make_async_copy(columns(ref, n), rows.at[n, at, :], row_sems.at[n, m])
                    for m, ref, at in spans(blocks)
                ]
            )
            for copy in row_copies[n]:
                copy.start()
        side = weights.at[
            pl.ds((n % half) * group, group), pl.ds((n // half) * depth, depth), :
        ]
        copies.append(pltpu.make_async_copy(side, held.at[n], sems.at[n]))
        copies[n].start()
    for n in range(half):
        for copy in row_copies[n]:
            copy.wait()
        copies[n].wait()
        part = jnp.dot(rows[n], held[n].reshape(block, -1), preferred_element_type=F32)
        acc[...] = part if n == 0 else acc[...] + part
    hidden = jnp.square(jnp.maximum(acc[...], 0.0)).astype(BF16)
    for n in range(half):
        copies[half + n].wait()
        ready[n] = mm_nt(hidden, held[half + n].reshape(block, -1)).astype(BF16)
        for m, ref, at in spans(outs):
            copy = pltpu.make_async_copy(ready.at[n, at, :], columns(ref, n), out_sems.at[n, m])
            copy.start()
            out_copies.append(copy)
    for copy in out_copies:
        copy.wait()


def channel(blocks, weights):
    peers, depth, hidden = weights.shape
    width = blocks[0].shape[1]
    total = sum(b.shape[0] for b in blocks)
    pieces = 8
    far = pl.BlockSpec(memory_space=pl.ANY)
    return pl.pallas_call(
        channel_kernel,
        in_specs=[far] * (len(blocks) + 1),
        out_specs=[far] * 4,
        out_shape=[
            jax.ShapeDtypeStruct((rows, width), BF16) for rows in (3 * total // 8, total // 8) * 2
        ],
        scratch_shapes=[
            pltpu.VMEM((pieces // 2, total, 2 * width // pieces), BF16),
            pltpu.VMEM((total, hidden), F32),
            pltpu.VMEM((pieces, 2 * peers // pieces, depth // 2, hidden), BF16),
            pltpu.VMEM((pieces // 2, total, 2 * width // pieces), BF16),
            pltpu.SemaphoreType.DMA((pieces // 2, len(blocks))),
            pltpu.SemaphoreType.DMA((pieces,)),
            pltpu.SemaphoreType.DMA((pieces // 2, 4)),
        ],
        cost_estimate=pl.CostEstimate(
            flops=4 * total * width * hidden,
            bytes_accessed=2 * peers * depth * hidden,
            transcendentals=0,
        ),
        name="channel",
    )(*blocks, weights)


def layer(
    stream,
    query_first,
    key_first,
    value_first,
    decay_first,
    learning_first,
    output_gate_first,
    extra_decay_first,
    head_norm_gain_first,
    self_weight_first,
    query_second,
    key_second,
    value_second,
    decay_second,
    learning_second,
    output_gate_second,
    extra_decay_second,
    head_norm_gain_second,
    self_weight_second,
    output_projection_first,
    output_projection_second,
    middle_norm_gain,
    mixer_up_weight,
    mixer_down_weight,
    final_norm_gain,
):
    count, _ = stream.shape
    both = jnp.concatenate([mixer_up_weight, mixer_down_weight.T], 0)
    weights = lax.all_gather(both, SP)

    solved, reads, begin_1, begin_2, sq1, sz1, sq2, sz2, total = chunk_maps(
        (query_first, key_first, value_first, decay_first, learning_first, extra_decay_first.T),
        (
            query_second,
            key_second,
            value_second,
            decay_second,
            learning_second,
            extra_decay_second.T,
        ),
    )
    entries = chunk_reads(
        solved, reads, begin_1, begin_2, value_first, value_second, sq1, sz1, sq2, sz2
    )
    prefix, (entry_1, inner_1, entry_2, inner_2) = sequence_prefix(total, entries)
    params = jnp.stack(
        [head_norm_gain_first, self_weight_first, head_norm_gain_second, self_weight_second]
    )
    mixer = mixer_outputs(
        prefix,
        (
            (entry_1, inner_1, query_first, key_first, value_first, output_gate_first),
            (entry_2, inner_2, query_second, key_second, value_second, output_gate_second),
        ),
        params,
    )
    rows = lax.all_to_all(mixer.reshape(-1, count, 2 * LANES), TP, 0, 0, tiled=True)
    middle = project(
        rows, output_projection_first, output_projection_second, stream, middle_norm_gain
    )

    nx = lax.axis_size("x")
    half = count // 2
    own_there = swap_core(middle)
    near_p = shift(middle, "x", 1, nx, True)
    near_m = shift(middle, "x", -1, nx, True)
    far = jnp.concatenate(
        [shift(near_p[:half], "x", 1, nx, True), shift(near_m[half:], "x", -1, nx, True)], 0
    )
    near = jnp.concatenate([near_p, near_m], 0)
    near_there = swap_core(near)
    far_there = swap_core(far)
    near_part, far_part, near_send, far_send = channel(
        (middle, near, far, own_there, near_there, far_there), weights
    )
    far_back = swap_core(far_send)
    near_back = swap_core(near_send)

    def total_of(part, back, n):
        at = slice(n * count, (n + 1) * count)
        return part[at].astype(F32) + back[at].astype(F32)

    from_far = shift(total_of(far_part, far_back, 0).astype(BF16), "x", 2, nx, True)
    from_p = shift(total_of(near_part, near_back, 1).astype(BF16), "x", -1, nx, True)
    from_m = shift(total_of(near_part, near_back, 2).astype(BF16), "x", 1, nx, True)
    ff_total = total_of(near_part, near_back, 0)
    for part in (from_far, from_p, from_m):
        ff_total = ff_total + part.astype(F32)
    return norm_rows(ALPHA * middle.astype(F32) + ff_total, final_norm_gain).astype(BF16)


def solution(mesh):
    split = Mesh(mesh.devices.reshape(8, 4, 4, 2), ALL)
    long = P(SP, TP)
    group = (long,) * 7 + (P(TP), P(TP))
    return jax.shard_map(
        layer,
        mesh=split,
        in_specs=(P(ALL, None),)
        + group
        + group
        + (P(), P(), P(), P(SP, TP), P(TP, SP), P()),
        out_specs=P(ALL, None),
        check_vma=False,
    )
```
